32 devices in a mesh: row: 8 (over z, x), col: 4 (over y, core).
Axes of the slice: x: 2, y: 2, z: 4, core: 2. Of those that a mesh axis runs over, the one named last changes fastest.
Arguments:
- tokens: bfloat16 [2048, 2048], P('row'), may hold values from -6 to 6
- norm_gain: float32 [2048], replicated, may hold values from 0.5 to 1.5
- first_gate: bfloat16 [2048, 1024], P(None, 'col'), may hold values from -0.125 to 0.125
- second_gate: bfloat16 [2048, 1024], P(None, 'col'), may hold values from -0.125 to 0.125
- value_weight: bfloat16 [2048, 1024], P(None, 'col'), may hold values from -0.125 to 0.125
- short_weight: bfloat16 [3, 3, 1024], P(None, None, 'col'), may hold values from -3.5 to 3.5
- short_bias: float32 [3, 1024], P(None, 'col'), may hold values from -2 to 2
- embed_weight: float32 [33, 64], replicated, may hold values from -1 to 1
- embed_bias: float32 [64], replicated, may hold values from -3 to 3
- inner_weight: float32 [64, 64], replicated, may hold values from -0.75 to 0.75
- inner_bias: float32 [64], replicated, may hold values from -3 to 3
- filter_freq: float32 [64], replicated, may hold values from 0.5 to 1.5
- filter_weight: float32 [2, 2, 64, 1024], P(None, None, None, ('col', 'row')), may hold values from -0.046875 to 0.046875
- filter_skip: float32 [2, 1024], P(None, ('col', 'row')), may hold values from -3 to 3
- output_gain: float32 [1024], P('col'), may hold values from 0.5 to 1.5
- output_weight: bfloat16 [1024, 2048], replicated, may hold values from -0.1875 to 0.1875
Outputs:
- mixed_output: bfloat16 [2048, 2048], P(('row', 'col'))
The draws below stay inside these ranges and needn't reach their ends.
All inputs are finite; a program needn't handle non-finite values.
Results may differ from the reference program's by a relative error of at most 0.01.
Values may be sent and summed in bfloat16 or wider, within the bound.
A program may use at most 64 MiB of HBM per device.

```python
import math
import jax
import jax.numpy as jnp
from jax import lax

MODEL_WIDTH = 2048
CHANNELS = 1024
GROUPS = 8
SHORT = 3
FREQ_BANDS = 16
FEATURES = 33
FILTER_HIDDEN = 64
SEQ_LEN = 2048


def shard_levels(key, dims, cuts, smallest, top_value):
    loudness = 1.0
    for dim, blocks in cuts:
        draws = jax.random.uniform(jax.random.fold_in(jax.random.fold_in(key, 6), dim), (blocks,), jnp.float32, smallest / len(cuts), top_value / len(cuts))
        loudness = loudness * jnp.repeat(jnp.exp(draws), dims[dim] // blocks).reshape((-1,) + (1,) * (len(dims) - 1 - dim))
    return loudness


def scatter_about(stream_key, shape, deviation, limit, cuts=(), held_as=jnp.bfloat16):
    array = deviation * jax.random.normal(stream_key, shape, jnp.float32)
    if cuts:
        array = array * shard_levels(stream_key, shape, cuts, -0.22, 0.18)
    return jnp.clip(array, -limit, limit).astype(held_as)


def setup_inputs(seed: int = 0) -> dict:
    key_of = jax.random.split(jax.random.key(seed), 17)
    return {
        "tokens": scatter_about(key_of[0], (SEQ_LEN, MODEL_WIDTH), 1.0, 6.0, ((0, 8),)),
        "norm_gain": jnp.clip(1.0 + 0.1 * jax.random.normal(key_of[1], (MODEL_WIDTH,), jnp.float32), 0.5, 1.5),
        "first_gate": scatter_about(key_of[2], (MODEL_WIDTH, CHANNELS), MODEL_WIDTH ** -0.5, 0.125, ((1, 4),)),
        "second_gate": scatter_about(key_of[3], (MODEL_WIDTH, CHANNELS), MODEL_WIDTH ** -0.5, 0.125, ((1, 4),)),
        "value_weight": scatter_about(key_of[4], (MODEL_WIDTH, CHANNELS), MODEL_WIDTH ** -0.5, 0.125, ((1, 4),)),
        "short_weight": scatter_about(key_of[5], (3, SHORT, CHANNELS), SHORT ** -0.5, 3.5, ((2, 4),)),
        "short_bias": scatter_about(key_of[6], (3, CHANNELS), 0.3, 2.0, ((1, 4),), jnp.float32),
        "embed_weight": scatter_about(key_of[7], (FEATURES, FILTER_HIDDEN), FEATURES ** -0.5, 1.0, (), jnp.float32),
        "embed_bias": scatter_about(key_of[8], (FILTER_HIDDEN,), 0.5, 3.0, (), jnp.float32),
        "inner_weight": scatter_about(key_of[9], (FILTER_HIDDEN, FILTER_HIDDEN), FILTER_HIDDEN ** -0.5, 0.75, (), jnp.float32),
        "inner_bias": scatter_about(key_of[10], (FILTER_HIDDEN,), 0.5, 3.0, (), jnp.float32),
        "filter_freq": jnp.clip(1.0 + 0.1 * jax.random.normal(key_of[11], (FILTER_HIDDEN,), jnp.float32), 0.5, 1.5),
        "filter_weight": scatter_about(key_of[12], (2, 2, FILTER_HIDDEN, CHANNELS), (FILTER_HIDDEN * SEQ_LEN // 8) ** -0.5, 0.046875, ((3, 32),), jnp.float32),
        "filter_skip": scatter_about(key_of[13], (2, CHANNELS), 0.5, 3.0, ((1, 32),), jnp.float32),
        "output_gain": jnp.clip(1.0 + 0.1 * jax.random.normal(key_of[14], (CHANNELS,), jnp.float32), 0.5, 1.5),
        "output_weight": scatter_about(key_of[15], (CHANNELS, MODEL_WIDTH), CHANNELS ** -0.5, 0.1875),
    }


HIGHEST = lax.Precision.HIGHEST
NORM_EPS = 1e-06
DECAY_TARGET = 0.01
FAST_SPAN = 0.3
SLOW_SPAN = 1.5

def position_features(length):
    position_ramp = jnp.linspace(0.0, 1.0, length, dtype=jnp.float32)[:, None]
    angles = 2.0 * math.pi * jnp.arange(length, dtype=jnp.float32)[:, None] / length
    band_freqs = jnp.linspace(0.0001, FREQ_BANDS - 1, FREQ_BANDS, dtype=jnp.float32)[None, :]
    features = jnp.concatenate([position_ramp, jnp.cos(band_freqs * angles), -jnp.sin(band_freqs * angles)], axis=1)
    return (position_ramp, features)

def filter_hidden(length, embed_weight, embed_bias, inner_weight, inner_bias, filter_freq):
    position_ramp, features = position_features(length)
    hidden = jnp.sin(filter_freq * (jnp.dot(features, embed_weight, precision=HIGHEST) + embed_bias))
    hidden = jnp.sin(filter_freq * (jnp.dot(hidden, inner_weight, precision=HIGHEST) + inner_bias))
    return (position_ramp, hidden)

def decay_rates():
    fastest = math.log(DECAY_TARGET) / FAST_SPAN
    slowest = math.log(DECAY_TARGET) / SLOW_SPAN
    return jnp.abs(jnp.linspace(slowest, fastest, CHANNELS, dtype=jnp.float32))

def short_filter(padded, weights, bias_row, length):
    result = bias_row.astype(jnp.float32)
    for tap_index in range(weights.shape[0]):
        result = result + padded[tap_index:tap_index + length].astype(jnp.float32) * weights[tap_index].astype(jnp.float32)
    return result

def two_sided(signal, forward, backward, skip_gain):
    length = signal.shape[0]
    circular_taps = jnp.concatenate([forward, jnp.zeros_like(forward[:1]), backward[:0:-1]], axis=0)
    spectrum = jnp.fft.rfft(signal, n=2 * length, axis=0) * jnp.fft.rfft(circular_taps, axis=0)
    return jnp.fft.irfft(spectrum, n=2 * length, axis=0)[:length] + signal * skip_gain

def reference(tokens, norm_gain, first_gate, second_gate, value_weight, short_weight, short_bias, embed_weight, embed_bias, inner_weight, inner_bias, filter_freq, filter_weight, filter_skip, output_gain, output_weight):
    widened = tokens.astype(jnp.float32)
    normed = (widened * lax.rsqrt(lax.optimization_barrier(jnp.mean(widened * widened, axis=1, keepdims=True)) + NORM_EPS) * norm_gain).astype(jnp.bfloat16)
    gate_first = jnp.dot(normed, first_gate, preferred_element_type=jnp.float32).astype(jnp.bfloat16)
    gate_second = jnp.dot(normed, second_gate, preferred_element_type=jnp.float32).astype(jnp.bfloat16)
    gate_value = jnp.dot(normed, value_weight, preferred_element_type=jnp.float32).astype(jnp.bfloat16)
    length = tokens.shape[0]
    position_ramp, hidden = filter_hidden(length, embed_weight, embed_bias, inner_weight, inner_bias, filter_freq)
    group_width = CHANNELS // GROUPS
    half_width = SHORT // 2

    def blocks(matrix):
        split = matrix.reshape(matrix.shape[:-1] + (GROUPS, group_width))
        return jnp.moveaxis(split, -2, 0)

    def one_block(pieces):
        first_block, second_block, value_block, weight_block, bias_block, filter_block, skip_block, decay_block, gain_block = pieces
        window = jnp.exp(-position_ramp * decay_block[None, :])
        smoothed = []
        for branch, source in enumerate((first_block, second_block, value_block)):
            padded = jnp.pad(source.astype(jnp.float32), ((half_width, SHORT - 1 - half_width), (0, 0)))
            smoothed.append(short_filter(padded, weight_block[branch], bias_block[branch], length))
        signal = smoothed[2]
        for order_index in range(2):
            forward = jnp.dot(hidden, filter_block[order_index, 0], precision=HIGHEST) * window
            backward = jnp.dot(hidden, filter_block[order_index, 1], precision=HIGHEST) * window
            signal = smoothed[order_index] * two_sided(signal, forward, backward, skip_block[order_index])
        scaled = signal * lax.rsqrt(lax.optimization_barrier(jnp.mean(signal * signal, axis=1, keepdims=True)) + NORM_EPS)
        return (scaled * gain_block).astype(jnp.bfloat16)
    normed_blocks = lax.map(one_block, (blocks(gate_first), blocks(gate_second), blocks(gate_value), blocks(short_weight), blocks(short_bias), blocks(filter_weight), blocks(filter_skip), blocks(decay_rates()), blocks(output_gain)))
    mixed = jnp.moveaxis(normed_blocks, 0, 1).reshape(length, CHANNELS)
    return jnp.dot(mixed, output_weight, preferred_element_type=jnp.float32).astype(jnp.bfloat16)
```

```python
import functools
import math

import jax
import jax.numpy as jnp
import numpy as np
from jax import lax
from jax.experimental import pallas as pl
from jax.experimental.pallas import tpu as pltpu
from jax.sharding import PartitionSpec as P

CHANNELS = 1024
GROUPS = 8
FREQ_BANDS = 16


HIGHEST = lax.Precision.HIGHEST
NORM_EPS = 1e-06
DECAY_TARGET = 0.01
FAST_SPAN = 0.3
SLOW_SPAN = 1.5


def for_sending(value):
    return jax.tree.map(lambda a: a.astype(jnp.bfloat16) if a.dtype == jnp.float32 else a, value)


def position_features(length):
    position_ramp = jnp.linspace(0.0, 1.0, length, dtype=jnp.float32)[:, None]
    angles = 2.0 * math.pi * jnp.arange(length, dtype=jnp.float32)[:, None] / length
    band_freqs = jnp.linspace(0.0001, FREQ_BANDS - 1, FREQ_BANDS, dtype=jnp.float32)[None, :]
    features = jnp.concatenate(
        [position_ramp, jnp.cos(band_freqs * angles), -jnp.sin(band_freqs * angles)], axis=1
    )
    return (position_ramp, features)


def filter_hidden(length, embed_weight, embed_bias, inner_weight, inner_bias, filter_freq):
    position_ramp, features = position_features(length)
    hidden = jnp.sin(
        filter_freq * (jnp.dot(features, embed_weight, precision=HIGHEST) + embed_bias)
    )
    hidden = jnp.sin(filter_freq * (jnp.dot(hidden, inner_weight, precision=HIGHEST) + inner_bias))
    return (position_ramp, hidden)


def decay_rates():
    fastest = math.log(DECAY_TARGET) / FAST_SPAN
    slowest = math.log(DECAY_TARGET) / SLOW_SPAN
    return jnp.abs(jnp.linspace(slowest, fastest, CHANNELS, dtype=jnp.float32))


def short_filter(padded, weights, bias_row, length):
    result = bias_row.astype(jnp.float32)
    for tap_index in range(weights.shape[0]):
        result = result + padded[tap_index : tap_index + length].astype(jnp.float32) * weights[
            tap_index
        ].astype(jnp.float32)
    return result


def phase_table(rows, cols, period):
    phase_index = (
        lax.broadcasted_iota(jnp.int32, (rows, cols), 0)
        * lax.broadcasted_iota(jnp.int32, (rows, cols), 1)
        % period
    )
    phase_angle = phase_index.astype(jnp.float32) * (2.0 * math.pi / period)
    return (jnp.cos(phase_angle), jnp.sin(phase_angle))


def split_length(total_size):
    chosen = 2
    for candidate in range(2, math.isqrt(total_size) + 1, 2):
        if total_size % candidate == 0:
            chosen = candidate
    return chosen


def make_tables(total_size):
    major_size = split_length(total_size)
    minor_size = total_size // major_size
    inner_table = phase_table(major_size, major_size, major_size)
    twiddle = phase_table(major_size, minor_size, total_size)
    outer_table = phase_table(minor_size, minor_size, minor_size)
    return (major_size, minor_size, inner_table, twiddle, outer_table)


def finish_forward(part_real, part_imag, twiddle, outer_table):
    turn_cos = twiddle[0][:, :, None]
    turn_sin = twiddle[1][:, :, None]
    turned_real = part_real * turn_cos + part_imag * turn_sin
    turned_imag = part_imag * turn_cos - part_real * turn_sin
    outer_cos, outer_sin = outer_table
    spec_real = jnp.einsum("anc,nk->akc", turned_real, outer_cos, precision=HIGHEST) + jnp.einsum(
        "anc,nk->akc", turned_imag, outer_sin, precision=HIGHEST
    )
    spec_imag = jnp.einsum("anc,nk->akc", turned_imag, outer_cos, precision=HIGHEST) - jnp.einsum(
        "anc,nk->akc", turned_real, outer_sin, precision=HIGHEST
    )
    return (spec_real, spec_imag)


def forward_signal(signal, tables):
    major_size, minor_size, inner_table, twiddle, outer_table = tables
    channels = signal.shape[1]
    flattened = signal.reshape(major_size // 2, minor_size * channels)
    inner_cos = inner_table[0][:, : major_size // 2]
    inner_sin = inner_table[1][:, : major_size // 2]
    part_real = jnp.dot(inner_cos, flattened, precision=HIGHEST).reshape(
        major_size, minor_size, channels
    )
    part_imag = -jnp.dot(inner_sin, flattened, precision=HIGHEST).reshape(
        major_size, minor_size, channels
    )
    return finish_forward(part_real, part_imag, twiddle, outer_table)


def forward_taps(circular_taps, tables):
    major_size, minor_size, inner_table, twiddle, outer_table = tables
    channels = circular_taps.shape[1]
    flattened = circular_taps.reshape(major_size, minor_size * channels)
    part_real = jnp.dot(inner_table[0], flattened, precision=HIGHEST).reshape(
        major_size, minor_size, channels
    )
    part_imag = -jnp.dot(inner_table[1], flattened, precision=HIGHEST).reshape(
        major_size, minor_size, channels
    )
    return finish_forward(part_real, part_imag, twiddle, outer_table)


def inverse(spec_real, spec_imag, tables):
    major_size, minor_size, inner_table, twiddle, outer_table = tables
    channels = spec_real.shape[2]
    outer_cos, outer_sin = outer_table
    back_real = jnp.einsum("akc,kn->anc", spec_real, outer_cos, precision=HIGHEST) - jnp.einsum(
        "akc,kn->anc", spec_imag, outer_sin, precision=HIGHEST
    )
    back_imag = jnp.einsum("akc,kn->anc", spec_imag, outer_cos, precision=HIGHEST) + jnp.einsum(
        "akc,kn->anc", spec_real, outer_sin, precision=HIGHEST
    )
    turn_cos = twiddle[0][:, :, None]
    turn_sin = twiddle[1][:, :, None]
    turned_real = (back_real * turn_cos - back_imag * turn_sin).reshape(
        major_size, minor_size * channels
    )
    turned_imag = (back_imag * turn_cos + back_real * turn_sin).reshape(
        major_size, minor_size * channels
    )
    half_rows = major_size // 2
    values = jnp.dot(inner_table[0][:half_rows], turned_real, precision=HIGHEST) - jnp.dot(
        inner_table[1][:half_rows], turned_imag, precision=HIGHEST
    )
    return values.reshape(half_rows * minor_size, channels) / (major_size * minor_size)


def two_sided(signal, forward, backward, skip_gain, tables):
    circular_taps = jnp.concatenate([forward, jnp.zeros_like(forward[:1]), backward[:0:-1]], axis=0)
    signal_real, signal_imag = forward_signal(signal, tables)
    taps_real, taps_imag = forward_taps(circular_taps, tables)
    prod_real = signal_real * taps_real - signal_imag * taps_imag
    prod_imag = signal_real * taps_imag + signal_imag * taps_real
    return inverse(prod_real, prod_imag, tables) + signal * skip_gain


def channel_taps(hidden, position_ramp, filter_weight, deltas):
    window = jnp.exp(-position_ramp * deltas[None, :])
    pairs = []
    for order_index in range(filter_weight.shape[0]):
        forward = jnp.dot(hidden, filter_weight[order_index, 0], precision=HIGHEST) * window
        backward = jnp.dot(hidden, filter_weight[order_index, 1], precision=HIGHEST) * window
        pairs.append((forward, backward))
    return pairs


def general_local(
    tokens,
    norm_gain,
    first_gate,
    second_gate,
    value_weight,
    short_weight,
    short_bias,
    embed_weight,
    embed_bias,
    inner_weight,
    inner_bias,
    filter_freq,
    filter_weight,
    filter_skip,
    output_gain,
    output_weight,
):
    row_count = lax.axis_size("row")
    row_index = lax.axis_index("row")
    col_index = lax.axis_index("col")
    local_tokens = tokens.shape[0]
    length = local_tokens * row_count
    col_width = first_gate.shape[1]
    own_width = col_width // row_count
    widened = tokens.astype(jnp.float32)
    normed = (
        widened
        * lax.rsqrt(jnp.mean(widened * widened, axis=1, keepdims=True) + NORM_EPS)
        * norm_gain
    ).astype(jnp.bfloat16)
    gate_first = jnp.dot(normed, first_gate, preferred_element_type=jnp.float32).astype(
        jnp.bfloat16
    )
    gate_second = jnp.dot(normed, second_gate, preferred_element_type=jnp.float32).astype(
        jnp.bfloat16
    )
    gate_value = jnp.dot(normed, value_weight, preferred_element_type=jnp.float32).astype(
        jnp.bfloat16
    )
    position_ramp, hidden = filter_hidden(
        length, embed_weight, embed_bias, inner_weight, inner_bias, filter_freq
    )
    channel_start = (col_index * row_count + row_index) * own_width
    deltas = lax.dynamic_slice_in_dim(decay_rates(), channel_start, own_width)
    tap_pairs = channel_taps(hidden, position_ramp, filter_weight, deltas)
    tables = make_tables(2 * length)
    half_width = short_weight.shape[1] // 2
    moved = (
        lax.all_to_all(gate_first, "row", split_axis=1, concat_axis=0, tiled=True),
        lax.all_to_all(gate_second, "row", split_axis=1, concat_axis=0, tiled=True),
        lax.all_to_all(gate_value, "row", split_axis=1, concat_axis=0, tiled=True),
    )
    weights_own = lax.dynamic_slice_in_dim(short_weight, row_index * own_width, own_width, 2)
    bias_own = lax.dynamic_slice_in_dim(short_bias, row_index * own_width, own_width, 1)
    smoothed = [
        short_filter(
            jnp.pad(moved[branch], ((half_width, half_width), (0, 0))),
            weights_own[branch],
            bias_own[branch],
            length,
        )
        for branch in range(3)
    ]
    signal = smoothed[2]
    for order_index in range(2):
        signal = smoothed[order_index] * two_sided(
            signal,
            tap_pairs[order_index][0],
            tap_pairs[order_index][1],
            filter_skip[order_index],
            tables,
        )
    result = jax.tree.map(
        lambda part, own: part.astype(own.dtype),
        lax.all_to_all(for_sending(signal), "row", split_axis=0, concat_axis=1, tiled=True),
        signal,
    )
    group_width = CHANNELS // GROUPS
    grouped = result.reshape(local_tokens, col_width // group_width, group_width)
    scaled = grouped * lax.rsqrt(jnp.mean(grouped * grouped, axis=2, keepdims=True) + NORM_EPS)
    mix_local = (scaled.reshape(local_tokens, col_width) * output_gain).astype(jnp.bfloat16)
    gathered = lax.all_to_all(mix_local, "col", split_axis=0, concat_axis=1, tiled=True)
    return jnp.dot(gathered, output_weight, preferred_element_type=jnp.float32).astype(jnp.bfloat16)


LANES = 128
SUBLANES = 16
BF16 = jnp.bfloat16
F32 = jnp.float32


def fast_tables(length, rows, tile_rows, own):
    total = 2 * length
    majors = length // LANES
    n1 = (np.arange(rows)[None, :] * tile_rows + np.arange(tile_rows)[:, None]).reshape(-1)
    k1 = np.arange(majors) + 0.5
    angle = 2.0 * np.pi * np.outer(k1, n1) / (2 * majors)
    eye = np.eye(own)
    inner = np.concatenate([np.kron(np.cos(angle), eye), np.kron(-np.sin(angle), eye)], 0)
    inner_back = inner.T * (2.0 / total)
    n2 = np.arange(LANES)
    turn = np.repeat(2.0 * np.pi * np.outer(k1, n2) / total, own, axis=0)
    twiddle = np.stack([np.cos(turn), np.sin(turn)])
    phase = 2.0 * np.pi * (np.outer(n2, n2) % LANES) / LANES
    c, s = np.cos(phase), np.sin(phase)
    outer = np.block([[c, -s], [s, c]])
    ramp = np.linspace(0.0, 1.0, length)
    angles = 2.0 * np.pi * np.arange(length) / length
    bands = np.linspace(0.0001, FREQ_BANDS - 1, FREQ_BANDS)[:, None]
    feats = np.concatenate([ramp[None], np.cos(bands * angles), -np.sin(bands * angles)], 0)
    return (
        jnp.asarray(inner, BF16),
        jnp.asarray(inner_back, BF16),
        jnp.asarray(twiddle, F32),
        jnp.asarray(outer, BF16),
        jnp.asarray(outer.T, BF16),
        jnp.asarray(feats, F32),
    )


def bounded_sin(x):
    turns = jnp.round(x * (1.0 / math.pi))
    r = x - turns * 3.140625
    r = r - turns * 9.67502593994140625e-4
    r = r - turns * 1.509957990978376432e-7
    half = turns * 0.5
    sign = 1.0 - 4.0 * (half - jnp.floor(half))
    q = r * r
    p = -2.5052108385e-8 + q * 1.6059043837e-10
    p = 2.7557319224e-6 + q * p
    p = -1.9841269841e-4 + q * p
    p = 8.3333333333e-3 + q * p
    p = -1.6666666667e-1 + q * p
    return sign * (r + r * q * p)


def mm(a, b):
    return jnp.dot(a.astype(BF16), b.astype(BF16), preferred_element_type=F32)


def tdot(a, b):
    return lax.dot_general(
        a, b, (((0,), (0,)), ((), ())), precision=HIGHEST, preferred_element_type=F32
    )


def column(row, start, count):
    shape = (count, row.shape[1])
    hit = lax.broadcasted_iota(jnp.int32, shape, 1) == start + lax.broadcasted_iota(
        jnp.int32, shape, 0
    )
    return jnp.sum(jnp.where(hit, row.astype(F32), 0.0), axis=1, keepdims=True)


def fast_kernel(
    dims,
    tokens_h,
    norm_gain,
    first_h,
    second_h,
    value_h,
    short_weight,
    short_bias,
    embed_weight,
    embed_bias,
    inner_weight,
    inner_bias,
    filter_freq,
    filter_weight,
    filter_skip,
    output_gain,
    out_w_h,
    inner_h,
    inner_back_h,
    twiddle_h,
    outer_h,
    outer_back_h,
    feats_h,
    out_ref,
    tokens_v,
    gates_v,
    out_w_v,
    inner_v,
    inner_back_v,
    twiddle_v,
    outer_v,
    outer_back_v,
    feats_v,
    normed_v,
    send_a,
    recv_a,
    send_b,
    recv_b,
    gains,
    gain_map,
    spectra,
    load_sem,
    send_a_sem,
    recv_a_sem,
    send_b_sem,
    recv_b_sem,
    send_g_sem,
    recv_g_sem,
):
    rows_n, cols_n, block, own = dims
    length = rows_n * block
    tiles = block // LANES
    piece = block // cols_n
    groups = LANES // piece
    half = own // groups
    row_me = lax.axis_index("row")
    col_me = lax.axis_index("col")
    me = row_me * cols_n + col_me
    everyone = rows_n * cols_n

    loads = [
        (tokens_h, tokens_v),
        (value_h, gates_v.at[2]),
        (first_h, gates_v.at[0]),
        (second_h, gates_v.at[1]),
        (feats_h, feats_v),
        (inner_h, inner_v),
        (twiddle_h, twiddle_v),
        (outer_h, outer_v),
        (outer_back_h, outer_back_v),
        (inner_back_h, inner_back_v),
    ] + [(out_w_h.at[:, g], out_w_v.at[g]) for g in range(groups)]
    copies = [
        pltpu.make_async_copy(src, dst, load_sem.at[i]) for i, (src, dst) in enumerate(loads)
    ]
    for copy in copies:
        copy.start()

    def place(flat):
        return (lax.div(flat, cols_n), lax.rem(flat, cols_n))

    barrier = pltpu.get_barrier_semaphore()
    for step in range(1, everyone):
        pl.semaphore_signal(
            barrier,
            inc=1,
            device_id=place(lax.rem(me + step, everyone)),
            device_id_type=pl.DeviceIdType.MESH,
        )

    copies[0].wait()
    gain_row = norm_gain[...]
    chunk = 32
    for start in range(0, block, chunk):
        x = tokens_v[start : start + chunk, :].astype(F32)
        scale = lax.rsqrt(jnp.mean(x * x, axis=1, keepdims=True) + NORM_EPS)
        normed_v[start : start + chunk, :] = (x * scale * gain_row).astype(BF16)

    sends = []
    for order, branch in enumerate((2, 0, 1)):
        copies[1 + order].wait()
        gate = jnp.dot(normed_v[...], gates_v[branch], preferred_element_type=F32)
        send_a[branch] = gate.T.astype(BF16).reshape(rows_n, own, block)
        if order == 0:
            pl.semaphore_wait(barrier, everyone - 1)
        for step in range(1, rows_n):
            peer = lax.rem(row_me + step, rows_n)
            copy = pltpu.make_async_remote_copy(
                src_ref=send_a.at[branch, peer],
                dst_ref=recv_a.at[branch, row_me],
                send_sem=send_a_sem.at[branch, step],
                recv_sem=recv_a_sem.at[branch, step],
                device_id=(peer, col_me),
                device_id_type=pl.DeviceIdType.MESH,
            )
            copy.start()
            sends.append((branch, copy))
        recv_a[branch, row_me] = send_a[branch, row_me]

    gain_sends = []
    gains[col_me] = output_gain[...]
    for step in range(1, cols_n):
        copy = pltpu.make_async_remote_copy(
            src_ref=output_gain,
            dst_ref=gains.at[col_me],
            send_sem=send_g_sem.at[step],
            recv_sem=recv_g_sem.at[step],
            device_id=(row_me, lax.rem(col_me + step, cols_n)),
            device_id_type=pl.DeviceIdType.MESH,
        )
        copy.start()
        gain_sends.append(copy)

    def to_layout(x):
        return jnp.concatenate(
            [
                jnp.concatenate(
                    [
                        x[:, g * half : (g + 1) * half, j * LANES : (j + 1) * LANES].reshape(
                            rows_n * half, LANES
                        )
                        for g in range(groups)
                    ],
                    axis=1,
                )
                for j in range(tiles)
            ],
            axis=0,
        )

    def taps_layout(x):
        return jnp.concatenate(
            [
                jnp.concatenate(
                    [
                        x[
                            g * half : (g + 1) * half,
                            (r * tiles + j) * LANES : (r * tiles + j + 1) * LANES,
                        ]
                        for g in range(groups)
                    ],
                    axis=1,
                )
                for j in range(tiles)
                for r in range(rows_n)
            ],
            axis=0,
        )

    freq = column(filter_freq[...], 0, filter_freq.shape[1])
    copies[4].wait()
    hidden = bounded_sin(
        freq
        * (
            tdot(embed_weight[...], feats_v[...])
            + column(embed_bias[...], 0, embed_bias.shape[1])
        )
    )
    hidden = bounded_sin(
        freq * (tdot(inner_weight[...], hidden) + column(inner_bias[...], 0, inner_bias.shape[1]))
    )
    channels = rows_n * cols_n * own
    slowest = math.log(DECAY_TARGET) / SLOW_SPAN
    fastest = math.log(DECAY_TARGET) / FAST_SPAN
    channel = (
        (col_me * rows_n + row_me) * own + lax.broadcasted_iota(jnp.int32, (own, 1), 0)
    ).astype(F32)
    decay = jnp.abs(slowest + channel * ((fastest - slowest) / (channels - 1)))
    lag = lax.broadcasted_iota(jnp.int32, (own, length), 1)
    window = jnp.exp(-(lag.astype(F32) * (1.0 / (length - 1))) * decay)
    for copy in copies[5:8]:
        copy.wait()

    def twist(real, imag, sign):
        cos = jnp.concatenate([twiddle_v[0]] * groups, axis=1)
        sin = jnp.concatenate([twiddle_v[1]] * groups, axis=1) * sign
        return real * cos + imag * sin, imag * cos - real * sin

    def lanes_of(x, g):
        return x[:, g * LANES : (g + 1) * LANES]

    def forward_inner(x):
        part = mm(inner_v[...], x)
        count = part.shape[0] // 2
        return twist(part[:count], part[count:], 1.0)

    for order in range(2):
        fwd = tdot(filter_weight[order, 0], hidden) * window
        bwd = jnp.where(lag == 0, 0.0, tdot(filter_weight[order, 1], hidden) * window)
        plus = forward_inner(taps_layout(fwd + bwd))
        minus = forward_inner(taps_layout(fwd - bwd))
        for g in range(groups):
            p = jnp.concatenate([lanes_of(plus[0], g), lanes_of(plus[1], g)], axis=1)
            m = jnp.concatenate([lanes_of(minus[0], g), lanes_of(minus[1], g)], axis=1)
            spectra[order, g, :, :LANES] = mm(p, outer_v[:, :LANES])
            spectra[order, g, :, LANES:] = mm(m, outer_v[:, LANES:])

    for copy in gain_sends:
        copy.wait_recv()
    lane = lax.broadcasted_iota(jnp.int32, (rows_n * half, LANES), 1)
    width = rows_n * own
    for q in range(cols_n):
        col_gain = column(gains[q], 0, width).reshape(rows_n, own, 1)
        result = jnp.zeros((rows_n * half, LANES), F32)
        for g in range(groups):
            part = col_gain[:, g * half : (g + 1) * half].reshape(rows_n * half, 1)
            result = jnp.where(lax.div(lane, piece) == g, part, result)
        gain_map[q] = result

    for copy in copies[8:10]:
        copy.wait()
    pos = lax.broadcasted_iota(jnp.int32, (rows_n, own, block), 2)

    def smooth(branch):
        for b, copy in sends:
            if b == branch:
                copy.wait_recv()
        x = recv_a[branch].astype(F32)
        flat = x.reshape(rows_n * own, block)
        before = pltpu.roll(flat, 1, 1).reshape(rows_n, own, block)
        after = pltpu.roll(flat, block - 1, 1).reshape(rows_n, own, block)
        gap = jnp.zeros((1, own, block), F32)
        before = jnp.where(pos == 0, jnp.concatenate([gap, before[:-1]], 0), before)
        after = jnp.where(pos == block - 1, jnp.concatenate([after[1:], gap], 0), after)
        start = row_me * own
        w = [
            column(short_weight[branch, j : j + 1, :], start, own).reshape(1, own, 1)
            for j in range(3)
        ]
        bias = column(short_bias[branch : branch + 1, :], start, own).reshape(1, own, 1)
        return to_layout(bias + before * w[0] + x * w[1] + after * w[2])

    signal = smooth(2)
    for order in range(2):
        real, imag = forward_inner(signal)
        back_real, back_imag = [], []
        for g in range(groups):
            t = jnp.concatenate([lanes_of(real, g), lanes_of(imag, g)], axis=1)
            spec = mm(t, outer_v[...])
            sr, si = spec[:, :LANES], spec[:, LANES:]
            hr, hi = spectra[order, g, :, :LANES], spectra[order, g, :, LANES:]
            prod = jnp.concatenate([sr * hr - si * hi, sr * hi + si * hr], axis=1)
            back = mm(prod, outer_back_v[...])
            back_real.append(back[:, :LANES])
            back_imag.append(back[:, LANES:])
        ur, ui = twist(jnp.concatenate(back_real, 1), jnp.concatenate(back_imag, 1), -1.0)
        conv = mm(inner_back_v[...], jnp.concatenate([ur, ui], axis=0))
        skip = column(filter_skip[order : order + 1, :], 0, own)
        skip = to_layout(jnp.broadcast_to(skip[None], (rows_n, own, block)))
        signal = smooth(order) * (conv + signal * skip)

    count = rows_n * half
    for j in range(tiles):
        for h in range(LANES // piece):
            part = jnp.concatenate(
                [
                    signal[
                        j * count : (j + 1) * count,
                        g * LANES + h * piece : g * LANES + (h + 1) * piece,
                    ]
                    for g in range(groups)
                ],
                axis=1,
            )
            send_b[j * (LANES // piece) + h] = part.astype(BF16).reshape(rows_n, half, LANES)
    last = []
    for step in range(1, everyone):
        row_to, col_to = place(lax.rem(me + step, everyone))
        copy = pltpu.make_async_remote_copy(
            src_ref=send_b.at[col_to, row_to],
            dst_ref=recv_b.at[col_me, row_me],
            send_sem=send_b_sem.at[step],
            recv_sem=recv_b_sem.at[step],
            device_id=(row_to, col_to),
            device_id_type=pl.DeviceIdType.MESH,
        )
        copy.start()
        last.append(copy)
    recv_b[col_me, row_me] = send_b[col_me, row_me]
    for copy in copies[10:]:
        copy.wait()
    for copy in last:
        copy.wait_recv()

    group_width = CHANNELS // GROUPS
    per_group = group_width // own
    turned = []
    for q in range(cols_n):
        for r in range(0, rows_n, per_group):
            x = recv_b[q, r : r + per_group].astype(F32).reshape(per_group * half, LANES)
            total = jnp.sum(x * x, axis=0, keepdims=True)
            square = total
            for g in range(1, groups):
                square = square + pltpu.roll(total, g * piece, 1)
            scale = lax.rsqrt(square * (1.0 / group_width) + NORM_EPS)
            gain = gain_map[q, r * half : (r + per_group) * half, :]
            turned.append(x * scale * gain)
    mixed = jnp.concatenate(turned, axis=0).T.astype(BF16)
    depth = everyone * half
    step_width = 512
    for start in range(0, out_ref.shape[1], step_width):
        acc = jnp.zeros((piece, step_width), F32)
        for g in range(groups):
            acc = acc + jnp.dot(
                mixed[g * piece : (g + 1) * piece],
                out_w_v[g, :, :, start : start + step_width].reshape(depth, step_width),
                preferred_element_type=F32,
            )
        out_ref[:, start : start + step_width] = acc.astype(BF16)

    for _, copy in sends:
        copy.wait_send()
    for copy in gain_sends + last:
        copy.wait_send()


def fast_local(*args):
    (
        tokens, norm_gain, first_gate, second_gate, value_weight, short_weight, short_bias,
        embed_weight, embed_bias, inner_weight, inner_bias, filter_freq, filter_weight,
        filter_skip, output_gain, output_weight,
    ) = args
    rows_n, cols_n = lax.axis_size("row"), lax.axis_size("col")
    block, model = tokens.shape
    own = filter_weight.shape[3]
    piece = block // cols_n
    groups = LANES // piece
    half = own // groups
    tiles = block // LANES
    length = block * rows_n
    width = first_gate.shape[1]
    everyone = rows_n * cols_n
    tables = fast_tables(length, rows_n, tiles, half)
    out_width = output_weight.shape[1]
    out_w = output_weight.reshape(everyone, groups, half, out_width)
    vm = pl.BlockSpec(memory_space=pltpu.VMEM)
    hbm = pl.BlockSpec(memory_space=pl.ANY)
    operands = [
        (tokens, hbm),
        (norm_gain.reshape(1, -1), vm),
        (first_gate, hbm),
        (second_gate, hbm),
        (value_weight, hbm),
        (short_weight, vm),
        (short_bias, vm),
        (embed_weight, vm),
        (embed_bias.reshape(1, -1), vm),
        (inner_weight, vm),
        (inner_bias.reshape(1, -1), vm),
        (filter_freq.reshape(1, -1), vm),
        (filter_weight, vm),
        (filter_skip, vm),
        (output_gain.reshape(1, -1), vm),
        (out_w, hbm),
    ] + [(table, hbm) for table in tables]
    rows_all = tiles * rows_n * half
    DMA = pltpu.SemaphoreType.DMA
    return pl.pallas_call(
        functools.partial(fast_kernel, (rows_n, cols_n, block, own)),
        out_shape=jax.ShapeDtypeStruct((piece, out_width), BF16),
        in_specs=[spec for _, spec in operands],
        out_specs=vm,
        scratch_shapes=[
            pltpu.VMEM(tokens.shape, BF16),
            pltpu.VMEM((3, model, width), BF16),
            pltpu.VMEM((groups, everyone, half, out_width), BF16),
        ]
        + [pltpu.VMEM(table.shape, table.dtype) for table in tables]
        + [
            pltpu.VMEM(tokens.shape, BF16),
            pltpu.VMEM((3, rows_n, own, block), BF16),
            pltpu.VMEM((3, rows_n, own, block), BF16),
            pltpu.VMEM((cols_n, rows_n, half, LANES), BF16),
            pltpu.VMEM((cols_n, rows_n, half, LANES), BF16),
            pltpu.VMEM((cols_n, 1, width), F32),
            pltpu.VMEM((cols_n, rows_n * half, LANES), F32),
            pltpu.VMEM((2, groups, rows_all, 2 * LANES), F32),
            DMA((10 + groups,)),
            DMA((3, rows_n)),
            DMA((3, rows_n)),
            DMA((everyone,)),
            DMA((everyone,)),
            DMA((cols_n,)),
            DMA((cols_n,)),
        ],
        compiler_params=pltpu.CompilerParams(
            collective_id=0, has_side_effects=True, vmem_limit_bytes=56 * 1024 * 1024
        ),
    )(*[operand for operand, _ in operands])


def kernel_fits(tokens, filter_weight, rows_n, cols_n):
    block = tokens.shape[0]
    own = filter_weight.shape[3]
    piece = block // cols_n
    if block % LANES or LANES % piece:
        return False
    groups = LANES // piece
    return own % (groups * SUBLANES) == 0 and (CHANNELS // GROUPS) % own == 0


def local(*args):
    if kernel_fits(args[0], args[12], lax.axis_size("row"), lax.axis_size("col")):
        return fast_local(*args)
    return general_local(*args)


def solution(mesh):
    in_specs = (
        P("row", None),
        P(),
        P(None, "col"),
        P(None, "col"),
        P(None, "col"),
        P(None, None, "col"),
        P(None, "col"),
        P(),
        P(),
        P(),
        P(),
        P(),
        P(None, None, None, ("col", "row")),
        P(None, ("col", "row")),
        P("col"),
        P(),
    )
    out_specs = P(("row", "col"), None)
    return jax.shard_map(local, mesh=mesh, in_specs=in_specs, out_specs=out_specs, check_vma=False)
```

```python
import functools
import math

import jax
import jax.numpy as jnp
import numpy as np
from jax import lax
from jax.experimental import pallas as pl
from jax.experimental.pallas import tpu as pltpu
from jax.sharding import PartitionSpec as P

CHANNELS = 1024
GROUPS = 8
FREQ_BANDS = 16


HIGHEST = lax.Precision.HIGHEST
NORM_EPS = 1e-06
DECAY_TARGET = 0.01
FAST_SPAN = 0.3
SLOW_SPAN = 1.5


def for_sending(value):
    return jax.tree.map(lambda a: a.astype(jnp.bfloat16) if a.dtype == jnp.float32 else a, value)


def position_features(length):
    position_ramp = jnp.linspace(0.0, 1.0, length, dtype=jnp.float32)[:, None]
    angles = 2.0 * math.pi * jnp.arange(length, dtype=jnp.float32)[:, None] / length
    band_freqs = jnp.linspace(0.0001, FREQ_BANDS - 1, FREQ_BANDS, dtype=jnp.float32)[None, :]
    features = jnp.concatenate(
        [position_ramp, jnp.cos(band_freqs * angles), -jnp.sin(band_freqs * angles)], axis=1
    )
    return (position_ramp, features)


def filter_hidden(length, embed_weight, embed_bias, inner_weight, inner_bias, filter_freq):
    position_ramp, features = position_features(length)
    hidden = jnp.sin(
        filter_freq * (jnp.dot(features, embed_weight, precision=HIGHEST) + embed_bias)
    )
    hidden = jnp.sin(filter_freq * (jnp.dot(hidden, inner_weight, precision=HIGHEST) + inner_bias))
    return (position_ramp, hidden)


def decay_rates():
    fastest = math.log(DECAY_TARGET) / FAST_SPAN
    slowest = math.log(DECAY_TARGET) / SLOW_SPAN
    return jnp.abs(jnp.linspace(slowest, fastest, CHANNELS, dtype=jnp.float32))


def short_filter(padded, weights, bias_row, length):
    result = bias_row.astype(jnp.float32)
    for tap_index in range(weights.shape[0]):
        result = result + padded[tap_index : tap_index + length].astype(jnp.float32) * weights[
            tap_index
        ].astype(jnp.float32)
    return result


def phase_table(rows, cols, period):
    phase_index = (
        lax.broadcasted_iota(jnp.int32, (rows, cols), 0)
        * lax.broadcasted_iota(jnp.int32, (rows, cols), 1)
        % period
    )
    phase_angle = phase_index.astype(jnp.float32) * (2.0 * math.pi / period)
    return (jnp.cos(phase_angle), jnp.sin(phase_angle))


def split_length(total_size):
    chosen = 2
    for candidate in range(2, math.isqrt(total_size) + 1, 2):
        if total_size % candidate == 0:
            chosen = candidate
    return chosen


def make_tables(total_size):
    major_size = split_length(total_size)
    minor_size = total_size // major_size
    inner_table = phase_table(major_size, major_size, major_size)
    twiddle = phase_table(major_size, minor_size, total_size)
    outer_table = phase_table(minor_size, minor_size, minor_size)
    return (major_size, minor_size, inner_table, twiddle, outer_table)


def finish_forward(part_real, part_imag, twiddle, outer_table):
    turn_cos = twiddle[0][:, :, None]
    turn_sin = twiddle[1][:, :, None]
    turned_real = part_real * turn_cos + part_imag * turn_sin
    turned_imag = part_imag * turn_cos - part_real * turn_sin
    outer_cos, outer_sin = outer_table
    spec_real = jnp.einsum("anc,nk->akc", turned_real, outer_cos, precision=HIGHEST) + jnp.einsum(
        "anc,nk->akc", turned_imag, outer_sin, precision=HIGHEST
    )
    spec_imag = jnp.einsum("anc,nk->akc", turned_imag, outer_cos, precision=HIGHEST) - jnp.einsum(
        "anc,nk->akc", turned_real, outer_sin, precision=HIGHEST
    )
    return (spec_real, spec_imag)


def forward_signal(signal, tables):
    major_size, minor_size, inner_table, twiddle, outer_table = tables
    channels = signal.shape[1]
    flattened = signal.reshape(major_size // 2, minor_size * channels)
    inner_cos = inner_table[0][:, : major_size // 2]
    inner_sin = inner_table[1][:, : major_size // 2]
    part_real = jnp.dot(inner_cos, flattened, precision=HIGHEST).reshape(
        major_size, minor_size, channels
    )
    part_imag = -jnp.dot(inner_sin, flattened, precision=HIGHEST).reshape(
        major_size, minor_size, channels
    )
    return finish_forward(part_real, part_imag, twiddle, outer_table)


def forward_taps(circular_taps, tables):
    major_size, minor_size, inner_table, twiddle, outer_table = tables
    channels = circular_taps.shape[1]
    flattened = circular_taps.reshape(major_size, minor_size * channels)
    part_real = jnp.dot(inner_table[0], flattened, precision=HIGHEST).reshape(
        major_size, minor_size, channels
    )
    part_imag = -jnp.dot(inner_table[1], flattened, precision=HIGHEST).reshape(
        major_size, minor_size, channels
    )
    return finish_forward(part_real, part_imag, twiddle, outer_table)


def inverse(spec_real, spec_imag, tables):
    major_size, minor_size, inner_table, twiddle, outer_table = tables
    channels = spec_real.shape[2]
    outer_cos, outer_sin = outer_table
    back_real = jnp.einsum("akc,kn->anc", spec_real, outer_cos, precision=HIGHEST) - jnp.einsum(
        "akc,kn->anc", spec_imag, outer_sin, precision=HIGHEST
    )
    back_imag = jnp.einsum("akc,kn->anc", spec_imag, outer_cos, precision=HIGHEST) + jnp.einsum(
        "akc,kn->anc", spec_real, outer_sin, precision=HIGHEST
    )
    turn_cos = twiddle[0][:, :, None]
    turn_sin = twiddle[1][:, :, None]
    turned_real = (back_real * turn_cos - back_imag * turn_sin).reshape(
        major_size, minor_size * channels
    )
    turned_imag = (back_imag * turn_cos + back_real * turn_sin).reshape(
        major_size, minor_size * channels
    )
    half_rows = major_size // 2
    values = jnp.dot(inner_table[0][:half_rows], turned_real, precision=HIGHEST) - jnp.dot(
        inner_table[1][:half_rows], turned_imag, precision=HIGHEST
    )
    return values.reshape(half_rows * minor_size, channels) / (major_size * minor_size)


def two_sided(signal, forward, backward, skip_gain, tables):
    circular_taps = jnp.concatenate([forward, jnp.zeros_like(forward[:1]), backward[:0:-1]], axis=0)
    signal_real, signal_imag = forward_signal(signal, tables)
    taps_real, taps_imag = forward_taps(circular_taps, tables)
    prod_real = signal_real * taps_real - signal_imag * taps_imag
    prod_imag = signal_real * taps_imag + signal_imag * taps_real
    return inverse(prod_real, prod_imag, tables) + signal * skip_gain


def channel_taps(hidden, position_ramp, filter_weight, deltas):
    window = jnp.exp(-position_ramp * deltas[None, :])
    pairs = []
    for order_index in range(filter_weight.shape[0]):
        forward = jnp.dot(hidden, filter_weight[order_index, 0], precision=HIGHEST) * window
        backward = jnp.dot(hidden, filter_weight[order_index, 1], precision=HIGHEST) * window
        pairs.append((forward, backward))
    return pairs


def general_local(
    tokens,
    norm_gain,
    first_gate,
    second_gate,
    value_weight,
    short_weight,
    short_bias,
    embed_weight,
    embed_bias,
    inner_weight,
    inner_bias,
    filter_freq,
    filter_weight,
    filter_skip,
    output_gain,
    output_weight,
):
    row_count = lax.axis_size("row")
    row_index = lax.axis_index("row")
    col_index = lax.axis_index("col")
    local_tokens = tokens.shape[0]
    length = local_tokens * row_count
    col_width = first_gate.shape[1]
    own_width = col_width // row_count
    widened = tokens.astype(jnp.float32)
    normed = (
        widened
        * lax.rsqrt(jnp.mean(widened * widened, axis=1, keepdims=True) + NORM_EPS)
        * norm_gain
    ).astype(jnp.bfloat16)
    gate_first = jnp.dot(normed, first_gate, preferred_element_type=jnp.float32).astype(
        jnp.bfloat16
    )
    gate_second = jnp.dot(normed, second_gate, preferred_element_type=jnp.float32).astype(
        jnp.bfloat16
    )
    gate_value = jnp.dot(normed, value_weight, preferred_element_type=jnp.float32).astype(
        jnp.bfloat16
    )
    position_ramp, hidden = filter_hidden(
        length, embed_weight, embed_bias, inner_weight, inner_bias, filter_freq
    )
    channel_start = (col_index * row_count + row_index) * own_width
    deltas = lax.dynamic_slice_in_dim(decay_rates(), channel_start, own_width)
    tap_pairs = channel_taps(hidden, position_ramp, filter_weight, deltas)
    tables = make_tables(2 * length)
    half_width = short_weight.shape[1] // 2
    moved = (
        lax.all_to_all(gate_first, "row", split_axis=1, concat_axis=0, tiled=True),
        lax.all_to_all(gate_second, "row", split_axis=1, concat_axis=0, tiled=True),
        lax.all_to_all(gate_value, "row", split_axis=1, concat_axis=0, tiled=True),
    )
    weights_own = lax.dynamic_slice_in_dim(short_weight, row_index * own_width, own_width, 2)
    bias_own = lax.dynamic_slice_in_dim(short_bias, row_index * own_width, own_width, 1)
    smoothed = [
        short_filter(
            jnp.pad(moved[branch], ((half_width, half_width), (0, 0))),
            weights_own[branch],
            bias_own[branch],
            length,
        )
        for branch in range(3)
    ]
    signal = smoothed[2]
    for order_index in range(2):
        signal = smoothed[order_index] * two_sided(
            signal,
            tap_pairs[order_index][0],
            tap_pairs[order_index][1],
            filter_skip[order_index],
            tables,
        )
    result = jax.tree.map(
        lambda part, own: part.astype(own.dtype),
        lax.all_to_all(for_sending(signal), "row", split_axis=0, concat_axis=1, tiled=True),
        signal,
    )
    group_width = CHANNELS // GROUPS
    grouped = result.reshape(local_tokens, col_width // group_width, group_width)
    scaled = grouped * lax.rsqrt(jnp.mean(grouped * grouped, axis=2, keepdims=True) + NORM_EPS)
    mix_local = (scaled.reshape(local_tokens, col_width) * output_gain).astype(jnp.bfloat16)
    gathered = lax.all_to_all(mix_local, "col", split_axis=0, concat_axis=1, tiled=True)
    return jnp.dot(gathered, output_weight, preferred_element_type=jnp.float32).astype(jnp.bfloat16)


LANES = 128
SUBLANES = 16
BF16 = jnp.bfloat16
F32 = jnp.float32


def fast_tables(length, rows, tile_rows, own):
    total = 2 * length
    majors = length // LANES
    n1 = (np.arange(rows)[None, :] * tile_rows + np.arange(tile_rows)[:, None]).reshape(-1)
    k1 = np.arange(majors) + 0.5
    angle = 2.0 * np.pi * np.outer(k1, n1) / (2 * majors)
    eye = np.eye(own)
    inner = np.concatenate([np.kron(np.cos(angle), eye), np.kron(-np.sin(angle), eye)], 0)
    inner_back = inner.T * (2.0 / total)
    n2 = np.arange(LANES)
    turn = np.repeat(2.0 * np.pi * np.outer(k1, n2) / total, own, axis=0)
    twiddle = np.stack([np.cos(turn), np.sin(turn)])
    phase = 2.0 * np.pi * (np.outer(n2, n2) % LANES) / LANES
    c, s = np.cos(phase), np.sin(phase)
    outer = np.block([[c, -s], [s, c]])
    ramp = np.linspace(0.0, 1.0, length)
    angles = 2.0 * np.pi * np.arange(length) / length
    bands = np.linspace(0.0001, FREQ_BANDS - 1, FREQ_BANDS)[:, None]
    feats = np.concatenate([ramp[None], np.cos(bands * angles), -np.sin(bands * angles)], 0)
    return (
        jnp.asarray(inner, BF16),
        jnp.asarray(inner_back, BF16),
        jnp.asarray(twiddle, F32),
        jnp.asarray(outer, BF16),
        jnp.asarray(outer.T, BF16),
        jnp.asarray(feats, F32),
    )


def bounded_sin(x):
    turns = jnp.round(x * (1.0 / math.pi))
    r = x - turns * 3.140625
    r = r - turns * 9.67502593994140625e-4
    r = r - turns * 1.509957990978376432e-7
    half = turns * 0.5
    sign = 1.0 - 4.0 * (half - jnp.floor(half))
    q = r * r
    p = -2.5052108385e-8 + q * 1.6059043837e-10
    p = 2.7557319224e-6 + q * p
    p = -1.9841269841e-4 + q * p
    p = 8.3333333333e-3 + q * p
    p = -1.6666666667e-1 + q * p
    return sign * (r + r * q * p)


def mm(a, b):
    return jnp.dot(a.astype(BF16), b.astype(BF16), preferred_element_type=F32)


def tdot(a, b):
    return lax.dot_general(
        a, b, (((0,), (0,)), ((), ())), precision=HIGHEST, preferred_element_type=F32
    )


def fdot(a, b):
    return jnp.dot(a, b, precision=HIGHEST, preferred_element_type=F32)


def column(row, start, count):
    shape = (count, row.shape[1])
    hit = lax.broadcasted_iota(jnp.int32, shape, 1) == start + lax.broadcasted_iota(
        jnp.int32, shape, 0
    )
    return jnp.sum(jnp.where(hit, row.astype(F32), 0.0), axis=1, keepdims=True)


SMALL = 11


def fast_kernel(dims, *refs):
    tokens_h, first_h, second_h, value_h, out_w_h = refs[:5]
    small_h = refs[5 : 5 + SMALL]
    inner_h, inner_back_h, twiddle_h, outer_h, outer_back_h, feats_h, out_ref = refs[
        5 + SMALL : 12 + SMALL
    ]
    tokens_v, gates_v, out_w_v = refs[12 + SMALL : 15 + SMALL]
    small_v = refs[15 + SMALL : 15 + 2 * SMALL]
    (
        norm_gain, short_weight, short_bias, embed_weight, embed_bias, inner_weight,
        inner_bias, filter_freq, filter_weight, filter_skip, output_gain,
    ) = small_v
    (
        inner_v, inner_back_v, twiddle_v, outer_v, outer_back_v, feats_v, normed_v,
        send_a, recv_a, send_b, recv_b, send_s, recv_s, second_v, send_h, recv_h, gains,
        gain_map, spectra, load_sem, small_sem, send_a_sem, recv_a_sem, send_b_sem,
        recv_b_sem, send_g_sem, recv_g_sem, send_s_sem, recv_s_sem, send_h_sem, recv_h_sem,
    ) = refs[15 + 2 * SMALL :]
    rows_n, cols_n, block, own = dims
    length = rows_n * block
    tiles = block // LANES
    piece = block // cols_n
    groups = LANES // piece
    half = own // groups
    row_me = lax.axis_index("row")
    col_me = lax.axis_index("col")
    me = row_me * cols_n + col_me
    everyone = rows_n * cols_n

    loads = [
        (tokens_h, tokens_v),
        (value_h, gates_v.at[2]),
        (first_h, gates_v.at[0]),
        (second_h, gates_v.at[1]),
        (feats_h, feats_v),
        (inner_h, inner_v),
        (twiddle_h, twiddle_v),
        (outer_h, outer_v),
        (outer_back_h, outer_back_v),
        (inner_back_h, inner_back_v),
    ] + [(out_w_h.at[:, g], out_w_v.at[g]) for g in range(groups)]
    copies = [
        pltpu.make_async_copy(src, dst, load_sem.at[i]) for i, (src, dst) in enumerate(loads)
    ]
    smalls = [
        pltpu.make_async_copy(src, dst, small_sem.at[i])
        for i, (src, dst) in enumerate(zip(small_h, small_v))
    ]
    copies[0].start()
    smalls[0].start()
    copies[1].start()

    def place(flat):
        return (lax.div(flat, cols_n), lax.rem(flat, cols_n))

    barrier = pltpu.get_barrier_semaphore()
    for step in range(1, everyone):
        pl.semaphore_signal(
            barrier,
            inc=1,
            device_id=place(lax.rem(me + step, everyone)),
            device_id_type=pl.DeviceIdType.MESH,
        )

    for copy in copies[2:10] + smalls[1:]:
        copy.start()
    copies[0].wait()
    smalls[0].wait()
    gain_row = norm_gain[...]
    chunk = 32
    for start in range(0, block, chunk):
        x = tokens_v[start : start + chunk, :].astype(F32)
        scale = lax.rsqrt(jnp.mean(x * x, axis=1, keepdims=True) + NORM_EPS)
        normed_v[start : start + chunk, :] = (x * scale * gain_row).astype(BF16)

    MESH = pl.DeviceIdType.MESH
    sends = []
    for order, branch in enumerate((2, 0)):
        copies[1 + order].wait()
        gate = jnp.dot(normed_v[...], gates_v[branch], preferred_element_type=F32)
        send_a[order] = gate.T.astype(BF16).reshape(rows_n, own, block)
        if order == 0:
            pl.semaphore_wait(barrier, everyone - 1)
        for step in range(1, rows_n):
            peer = lax.rem(row_me + step, rows_n)
            copy = pltpu.make_async_remote_copy(
                src_ref=send_a.at[order, peer],
                dst_ref=recv_a.at[order, row_me],
                send_sem=send_a_sem.at[order, step],
                recv_sem=recv_a_sem.at[order, step],
                device_id=(peer, col_me),
                device_id_type=MESH,
            )
            copy.start()
            sends.append((order, copy))
        recv_a[order, row_me] = send_a[order, row_me]

    for copy in copies[10:]:
        copy.start()
    copies[3].wait()
    gate = jnp.dot(normed_v[...], gates_v[1], preferred_element_type=F32)
    gate = gate.astype(BF16).astype(F32)
    second_v[...] = gate.T
    send_h[0] = gate[:1]
    send_h[1] = gate[block - 1 :]
    halo_sends = []
    for edge, shift in ((0, rows_n - 1), (1, 1)):
        copy = pltpu.make_async_remote_copy(
            src_ref=send_h.at[edge],
            dst_ref=recv_h.at[edge],
            send_sem=send_h_sem.at[edge],
            recv_sem=recv_h_sem.at[edge],
            device_id=(lax.rem(row_me + shift, rows_n), col_me),
            device_id_type=MESH,
        )
        copy.start()
        halo_sends.append(copy)
    for copy in smalls[1:]:
        copy.wait()

    gain_sends = []
    gains[col_me] = output_gain[...]
    for step in range(1, cols_n):
        copy = pltpu.make_async_remote_copy(
            src_ref=output_gain,
            dst_ref=gains.at[col_me],
            send_sem=send_g_sem.at[step],
            recv_sem=recv_g_sem.at[step],
            device_id=(row_me, lax.rem(col_me + step, cols_n)),
            device_id_type=pl.DeviceIdType.MESH,
        )
        copy.start()
        gain_sends.append(copy)

    def to_layout(x):
        return jnp.concatenate(
            [
                jnp.concatenate(
                    [
                        x[:, g * half : (g + 1) * half, j * LANES : (j + 1) * LANES].reshape(
                            rows_n * half, LANES
                        )
                        for g in range(groups)
                    ],
                    axis=1,
                )
                for j in range(tiles)
            ],
            axis=0,
        )

    def taps_layout(x):
        return jnp.concatenate(
            [
                jnp.concatenate(
                    [
                        x[
                            g * half : (g + 1) * half,
                            (r * tiles + j) * LANES : (r * tiles + j + 1) * LANES,
                        ]
                        for g in range(groups)
                    ],
                    axis=1,
                )
                for j in range(tiles)
                for r in range(rows_n)
            ],
            axis=0,
        )

    freq = column(filter_freq[...], 0, filter_freq.shape[1])
    copies[4].wait()
    hidden = bounded_sin(
        freq
        * (
            tdot(embed_weight[...], feats_v[...])
            + column(embed_bias[...], 0, embed_bias.shape[1])
        )
    )
    hidden = bounded_sin(
        freq * (tdot(inner_weight[...], hidden) + column(inner_bias[...], 0, inner_bias.shape[1]))
    )
    channels = rows_n * cols_n * own
    slowest = math.log(DECAY_TARGET) / SLOW_SPAN
    fastest = math.log(DECAY_TARGET) / FAST_SPAN
    channel = (
        (col_me * rows_n + row_me) * own + lax.broadcasted_iota(jnp.int32, (own, 1), 0)
    ).astype(F32)
    decay = jnp.abs(slowest + channel * ((fastest - slowest) / (channels - 1)))
    lag = lax.broadcasted_iota(jnp.int32, (own, length), 1)
    window = jnp.exp(-(lag.astype(F32) * (1.0 / (length - 1))) * decay)
    for copy in copies[5:8]:
        copy.wait()

    def twist(real, imag, sign):
        cos = jnp.concatenate([twiddle_v[0]] * groups, axis=1)
        sin = jnp.concatenate([twiddle_v[1]] * groups, axis=1) * sign
        return real * cos + imag * sin, imag * cos - real * sin

    def lanes_of(x, g):
        return x[:, g * LANES : (g + 1) * LANES]

    def forward_inner(x):
        part = mm(inner_v[...], x)
        count = part.shape[0] // 2
        return twist(part[:count], part[count:], 1.0)

    for order in range(2):
        fwd = fdot(filter_weight[order, 0], hidden) * window
        bwd = jnp.where(lag == 0, 0.0, fdot(filter_weight[order, 1], hidden) * window)
        plus = forward_inner(taps_layout(fwd + bwd))
        minus = forward_inner(taps_layout(fwd - bwd))
        for g in range(groups):
            p = jnp.concatenate([lanes_of(plus[0], g), lanes_of(plus[1], g)], axis=1)
            m = jnp.concatenate([lanes_of(minus[0], g), lanes_of(minus[1], g)], axis=1)
            spectra[order, g, :, :LANES] = mm(p, outer_v[:, :LANES])
            spectra[order, g, :, LANES:] = mm(m, outer_v[:, LANES:])

    for copy in halo_sends:
        copy.wait_recv()
    width = rows_n * own
    count = rows_n * half
    x = second_v[...]
    spot = lax.broadcasted_iota(jnp.int32, (width, block), 1)
    first_col = jnp.where(row_me == 0, 0.0, column(recv_h[1], 0, width))
    last_col = jnp.where(row_me == rows_n - 1, 0.0, column(recv_h[0], 0, width))
    before = jnp.where(spot == 0, first_col, pltpu.roll(x, 1, 1))
    after = jnp.where(spot == block - 1, last_col, pltpu.roll(x, block - 1, 1))
    w = [column(short_weight[1, j : j + 1, :], 0, width) for j in range(3)]
    x = column(short_bias[1:2, :], 0, width) + before * w[0] + x * w[1] + after * w[2]
    x = x.reshape(rows_n, groups, half, block)
    for q in range(cols_n):
        part = jnp.concatenate(
            [x[:, g, :, q * piece : (q + 1) * piece].reshape(count, piece) for g in range(groups)],
            axis=1,
        )
        send_s[q] = part.astype(BF16)
    recv_s[col_me] = send_s[col_me]
    second_sends = []
    for step in range(1, cols_n):
        peer = lax.rem(col_me + step, cols_n)
        copy = pltpu.make_async_remote_copy(
            src_ref=send_s.at[peer],
            dst_ref=recv_s.at[col_me],
            send_sem=send_s_sem.at[step],
            recv_sem=recv_s_sem.at[step],
            device_id=(row_me, peer),
            device_id_type=MESH,
        )
        copy.start()
        second_sends.append(copy)

    for copy in gain_sends:
        copy.wait_recv()
    lane = lax.broadcasted_iota(jnp.int32, (rows_n * half, LANES), 1)
    for q in range(cols_n):
        col_gain = column(gains[q], 0, width).reshape(rows_n, own, 1)
        result = jnp.zeros((rows_n * half, LANES), F32)
        for g in range(groups):
            part = col_gain[:, g * half : (g + 1) * half].reshape(rows_n * half, 1)
            result = jnp.where(lax.div(lane, piece) == g, part, result)
        gain_map[q] = result

    for copy in copies[8:10]:
        copy.wait()
    pos = lax.broadcasted_iota(jnp.int32, (rows_n, own, block), 2)

    def smooth(slot, branch):
        for b, copy in sends:
            if b == slot:
                copy.wait_recv()
        x = recv_a[slot].astype(F32)
        flat = x.reshape(rows_n * own, block)
        before = pltpu.roll(flat, 1, 1).reshape(rows_n, own, block)
        after = pltpu.roll(flat, block - 1, 1).reshape(rows_n, own, block)
        gap = jnp.zeros((1, own, block), F32)
        before = jnp.where(pos == 0, jnp.concatenate([gap, before[:-1]], 0), before)
        after = jnp.where(pos == block - 1, jnp.concatenate([after[1:], gap], 0), after)
        start = row_me * own
        w = [
            column(short_weight[branch, j : j + 1, :], start, own).reshape(1, own, 1)
            for j in range(3)
        ]
        bias = column(short_bias[branch : branch + 1, :], start, own).reshape(1, own, 1)
        return to_layout(bias + before * w[0] + x * w[1] + after * w[2])

    signal = smooth(0, 2)
    for order in range(2):
        real, imag = forward_inner(signal)
        back_real, back_imag = [], []
        for g in range(groups):
            t = jnp.concatenate([lanes_of(real, g), lanes_of(imag, g)], axis=1)
            spec = mm(t, outer_v[...])
            sr, si = spec[:, :LANES], spec[:, LANES:]
            hr, hi = spectra[order, g, :, :LANES], spectra[order, g, :, LANES:]
            prod = jnp.concatenate([sr * hr - si * hi, sr * hi + si * hr], axis=1)
            back = mm(prod, outer_back_v[...])
            back_real.append(back[:, :LANES])
            back_imag.append(back[:, LANES:])
        ur, ui = twist(jnp.concatenate(back_real, 1), jnp.concatenate(back_imag, 1), -1.0)
        conv = mm(inner_back_v[...], jnp.concatenate([ur, ui], axis=0))
        skip = column(filter_skip[order : order + 1, :], 0, own)
        skip = to_layout(jnp.broadcast_to(skip[None], (rows_n, own, block)))
        signal = conv + signal * skip
        if order == 0:
            signal = signal * smooth(1, 0)

    for j in range(tiles):
        for h in range(LANES // piece):
            part = jnp.concatenate(
                [
                    signal[
                        j * count : (j + 1) * count,
                        g * LANES + h * piece : g * LANES + (h + 1) * piece,
                    ]
                    for g in range(groups)
                ],
                axis=1,
            )
            send_b[j * (LANES // piece) + h] = part.astype(BF16).reshape(rows_n, half, LANES)
    last = []
    for step in range(1, everyone):
        row_to, col_to = place(lax.rem(me + step, everyone))
        copy = pltpu.make_async_remote_copy(
            src_ref=send_b.at[col_to, row_to],
            dst_ref=recv_b.at[col_me, row_me],
            send_sem=send_b_sem.at[step],
            recv_sem=recv_b_sem.at[step],
            device_id=(row_to, col_to),
            device_id_type=pl.DeviceIdType.MESH,
        )
        copy.start()
        last.append(copy)
    recv_b[col_me, row_me] = send_b[col_me, row_me]
    for copy in copies[10:]:
        copy.wait()
    for copy in second_sends + last:
        copy.wait_recv()

    group_width = CHANNELS // GROUPS
    per_group = group_width // own
    turned = []
    for q in range(cols_n):
        for r in range(0, rows_n, per_group):
            x = recv_b[q, r : r + per_group].astype(F32).reshape(per_group * half, LANES)
            x = x * recv_s[q, r * half : (r + per_group) * half, :].astype(F32)
            total = jnp.sum(x * x, axis=0, keepdims=True)
            square = total
            for g in range(1, groups):
                square = square + pltpu.roll(total, g * piece, 1)
            scale = lax.rsqrt(square * (1.0 / group_width) + NORM_EPS)
            gain = gain_map[q, r * half : (r + per_group) * half, :]
            turned.append(x * scale * gain)
    mixed = jnp.concatenate(turned, axis=0).T.astype(BF16)
    depth = everyone * half
    step_width = 512
    for start in range(0, out_ref.shape[1], step_width):
        acc = jnp.zeros((piece, step_width), F32)
        for g in range(groups):
            acc = acc + jnp.dot(
                mixed[g * piece : (g + 1) * piece],
                out_w_v[g, :, :, start : start + step_width].reshape(depth, step_width),
                preferred_element_type=F32,
            )
        out_ref[:, start : start + step_width] = acc.astype(BF16)

    for _, copy in sends:
        copy.wait_send()
    for copy in halo_sends + gain_sends + second_sends + last:
        copy.wait_send()


def fast_local(*args):
    (
        tokens, norm_gain, first_gate, second_gate, value_weight, short_weight, short_bias,
        embed_weight, embed_bias, inner_weight, inner_bias, filter_freq, filter_weight,
        filter_skip, output_gain, output_weight,
    ) = args
    rows_n, cols_n = lax.axis_size("row"), lax.axis_size("col")
    block, model = tokens.shape
    own = filter_weight.shape[3]
    piece = block // cols_n
    groups = LANES // piece
    half = own // groups
    tiles = block // LANES
    length = block * rows_n
    width = first_gate.shape[1]
    everyone = rows_n * cols_n
    tables = fast_tables(length, rows_n, tiles, half)
    out_width = output_weight.shape[1]
    out_w = output_weight.reshape(everyone, groups, half, out_width)
    vm = pl.BlockSpec(memory_space=pltpu.VMEM)
    hbm = pl.BlockSpec(memory_space=pl.ANY)
    small = [
        norm_gain.reshape(1, -1),
        short_weight,
        short_bias,
        embed_weight,
        embed_bias.reshape(1, -1),
        inner_weight,
        inner_bias.reshape(1, -1),
        filter_freq.reshape(1, -1),
        jnp.swapaxes(filter_weight, 2, 3),
        filter_skip,
        output_gain.reshape(1, -1),
    ]
    operands = [tokens, first_gate, second_gate, value_weight, out_w, *small, *tables]
    rows_all = tiles * rows_n * half
    DMA = pltpu.SemaphoreType.DMA
    return pl.pallas_call(
        functools.partial(fast_kernel, (rows_n, cols_n, block, own)),
        out_shape=jax.ShapeDtypeStruct((piece, out_width), BF16),
        in_specs=[hbm] * len(operands),
        out_specs=vm,
        scratch_shapes=[
            pltpu.VMEM(tokens.shape, BF16),
            pltpu.VMEM((3, model, width), BF16),
            pltpu.VMEM((groups, everyone, half, out_width), BF16),
        ]
        + [pltpu.VMEM(array.shape, array.dtype) for array in small + list(tables)]
        + [
            pltpu.VMEM(tokens.shape, BF16),
            pltpu.VMEM((2, rows_n, own, block), BF16),
            pltpu.VMEM((2, rows_n, own, block), BF16),
            pltpu.VMEM((cols_n, rows_n, half, LANES), BF16),
            pltpu.VMEM((cols_n, rows_n, half, LANES), BF16),
            pltpu.VMEM((cols_n, rows_n * half, LANES), BF16),
            pltpu.VMEM((cols_n, rows_n * half, LANES), BF16),
            pltpu.VMEM((width, block), F32),
            pltpu.VMEM((2, 1, width), F32),
            pltpu.VMEM((2, 1, width), F32),
            pltpu.VMEM((cols_n, 1, width), F32),
            pltpu.VMEM((cols_n, rows_n * half, LANES), F32),
            pltpu.VMEM((2, groups, rows_all, 2 * LANES), F32),
            DMA((10 + groups,)),
            DMA((SMALL,)),
            DMA((2, rows_n)),
            DMA((2, rows_n)),
            DMA((everyone,)),
            DMA((everyone,)),
            DMA((cols_n,)),
            DMA((cols_n,)),
            DMA((cols_n,)),
            DMA((cols_n,)),
            DMA((2,)),
            DMA((2,)),
        ],
        compiler_params=pltpu.CompilerParams(
            collective_id=0, has_side_effects=True, vmem_limit_bytes=56 * 1024 * 1024
        ),
    )(*operands)


def kernel_fits(tokens, filter_weight, rows_n, cols_n):
    block = tokens.shape[0]
    own = filter_weight.shape[3]
    piece = block // cols_n
    if block % LANES or LANES % piece:
        return False
    groups = LANES // piece
    return own % (groups * SUBLANES) == 0 and (CHANNELS // GROUPS) % own == 0


def local(*args):
    if kernel_fits(args[0], args[12], lax.axis_size("row"), lax.axis_size("col")):
        return fast_local(*args)
    return general_local(*args)


def solution(mesh):
    in_specs = (
        P("row", None),
        P(),
        P(None, "col"),
        P(None, "col"),
        P(None, "col"),
        P(None, None, "col"),
        P(None, "col"),
        P(),
        P(),
        P(),
        P(),
        P(),
        P(None, None, None, ("col", "row")),
        P(None, ("col", "row")),
        P("col"),
        P(),
    )
    out_specs = P(("row", "col"), None)
    return jax.shard_map(local, mesh=mesh, in_specs=in_specs, out_specs=out_specs, check_vma=False)
```

```python
import functools
import math

import jax
import jax.numpy as jnp
import numpy as np
from jax import lax
from jax.experimental import pallas as pl
from jax.experimental.pallas import tpu as pltpu
from jax.sharding import PartitionSpec as P

CHANNELS = 1024
GROUPS = 8
FREQ_BANDS = 16


HIGHEST = lax.Precision.HIGHEST
NORM_EPS = 1e-06
DECAY_TARGET = 0.01
FAST_SPAN = 0.3
SLOW_SPAN = 1.5


def for_sending(value):
    return jax.tree.map(lambda a: a.astype(jnp.bfloat16) if a.dtype == jnp.float32 else a, value)


def position_features(length):
    position_ramp = jnp.linspace(0.0, 1.0, length, dtype=jnp.float32)[:, None]
    angles = 2.0 * math.pi * jnp.arange(length, dtype=jnp.float32)[:, None] / length
    band_freqs = jnp.linspace(0.0001, FREQ_BANDS - 1, FREQ_BANDS, dtype=jnp.float32)[None, :]
    features = jnp.concatenate(
        [position_ramp, jnp.cos(band_freqs * angles), -jnp.sin(band_freqs * angles)], axis=1
    )
    return (position_ramp, features)


def filter_hidden(length, embed_weight, embed_bias, inner_weight, inner_bias, filter_freq):
    position_ramp, features = position_features(length)
    hidden = jnp.sin(
        filter_freq * (jnp.dot(features, embed_weight, precision=HIGHEST) + embed_bias)
    )
    hidden = jnp.sin(filter_freq * (jnp.dot(hidden, inner_weight, precision=HIGHEST) + inner_bias))
    return (position_ramp, hidden)


def decay_rates():
    fastest = math.log(DECAY_TARGET) / FAST_SPAN
    slowest = math.log(DECAY_TARGET) / SLOW_SPAN
    return jnp.abs(jnp.linspace(slowest, fastest, CHANNELS, dtype=jnp.float32))


def short_filter(padded, weights, bias_row, length):
    result = bias_row.astype(jnp.float32)
    for tap_index in range(weights.shape[0]):
        result = result + padded[tap_index : tap_index + length].astype(jnp.float32) * weights[
            tap_index
        ].astype(jnp.float32)
    return result


def phase_table(rows, cols, period):
    phase_index = (
        lax.broadcasted_iota(jnp.int32, (rows, cols), 0)
        * lax.broadcasted_iota(jnp.int32, (rows, cols), 1)
        % period
    )
    phase_angle = phase_index.astype(jnp.float32) * (2.0 * math.pi / period)
    return (jnp.cos(phase_angle), jnp.sin(phase_angle))


def split_length(total_size):
    chosen = 2
    for candidate in range(2, math.isqrt(total_size) + 1, 2):
        if total_size % candidate == 0:
            chosen = candidate
    return chosen


def make_tables(total_size):
    major_size = split_length(total_size)
    minor_size = total_size // major_size
    inner_table = phase_table(major_size, major_size, major_size)
    twiddle = phase_table(major_size, minor_size, total_size)
    outer_table = phase_table(minor_size, minor_size, minor_size)
    return (major_size, minor_size, inner_table, twiddle, outer_table)


def finish_forward(part_real, part_imag, twiddle, outer_table):
    turn_cos = twiddle[0][:, :, None]
    turn_sin = twiddle[1][:, :, None]
    turned_real = part_real * turn_cos + part_imag * turn_sin
    turned_imag = part_imag * turn_cos - part_real * turn_sin
    outer_cos, outer_sin = outer_table
    spec_real = jnp.einsum("anc,nk->akc", turned_real, outer_cos, precision=HIGHEST) + jnp.einsum(
        "anc,nk->akc", turned_imag, outer_sin, precision=HIGHEST
    )
    spec_imag = jnp.einsum("anc,nk->akc", turned_imag, outer_cos, precision=HIGHEST) - jnp.einsum(
        "anc,nk->akc", turned_real, outer_sin, precision=HIGHEST
    )
    return (spec_real, spec_imag)


def forward_signal(signal, tables):
    major_size, minor_size, inner_table, twiddle, outer_table = tables
    channels = signal.shape[1]
    flattened = signal.reshape(major_size // 2, minor_size * channels)
    inner_cos = inner_table[0][:, : major_size // 2]
    inner_sin = inner_table[1][:, : major_size // 2]
    part_real = jnp.dot(inner_cos, flattened, precision=HIGHEST).reshape(
        major_size, minor_size, channels
    )
    part_imag = -jnp.dot(inner_sin, flattened, precision=HIGHEST).reshape(
        major_size, minor_size, channels
    )
    return finish_forward(part_real, part_imag, twiddle, outer_table)


def forward_taps(circular_taps, tables):
    major_size, minor_size, inner_table, twiddle, outer_table = tables
    channels = circular_taps.shape[1]
    flattened = circular_taps.reshape(major_size, minor_size * channels)
    part_real = jnp.dot(inner_table[0], flattened, precision=HIGHEST).reshape(
        major_size, minor_size, channels
    )
    part_imag = -jnp.dot(inner_table[1], flattened, precision=HIGHEST).reshape(
        major_size, minor_size, channels
    )
    return finish_forward(part_real, part_imag, twiddle, outer_table)


def inverse(spec_real, spec_imag, tables):
    major_size, minor_size, inner_table, twiddle, outer_table = tables
    channels = spec_real.shape[2]
    outer_cos, outer_sin = outer_table
    back_real = jnp.einsum("akc,kn->anc", spec_real, outer_cos, precision=HIGHEST) - jnp.einsum(
        "akc,kn->anc", spec_imag, outer_sin, precision=HIGHEST
    )
    back_imag = jnp.einsum("akc,kn->anc", spec_imag, outer_cos, precision=HIGHEST) + jnp.einsum(
        "akc,kn->anc", spec_real, outer_sin, precision=HIGHEST
    )
    turn_cos = twiddle[0][:, :, None]
    turn_sin = twiddle[1][:, :, None]
    turned_real = (back_real * turn_cos - back_imag * turn_sin).reshape(
        major_size, minor_size * channels
    )
    turned_imag = (back_imag * turn_cos + back_real * turn_sin).reshape(
        major_size, minor_size * channels
    )
    half_rows = major_size // 2
    values = jnp.dot(inner_table[0][:half_rows], turned_real, precision=HIGHEST) - jnp.dot(
        inner_table[1][:half_rows], turned_imag, precision=HIGHEST
    )
    return values.reshape(half_rows * minor_size, channels) / (major_size * minor_size)


def two_sided(signal, forward, backward, skip_gain, tables):
    circular_taps = jnp.concatenate([forward, jnp.zeros_like(forward[:1]), backward[:0:-1]], axis=0)
    signal_real, signal_imag = forward_signal(signal, tables)
    taps_real, taps_imag = forward_taps(circular_taps, tables)
    prod_real = signal_real * taps_real - signal_imag * taps_imag
    prod_imag = signal_real * taps_imag + signal_imag * taps_real
    return inverse(prod_real, prod_imag, tables) + signal * skip_gain


def channel_taps(hidden, position_ramp, filter_weight, deltas):
    window = jnp.exp(-position_ramp * deltas[None, :])
    pairs = []
    for order_index in range(filter_weight.shape[0]):
        forward = jnp.dot(hidden, filter_weight[order_index, 0], precision=HIGHEST) * window
        backward = jnp.dot(hidden, filter_weight[order_index, 1], precision=HIGHEST) * window
        pairs.append((forward, backward))
    return pairs


def general_local(
    tokens,
    norm_gain,
    first_gate,
    second_gate,
    value_weight,
    short_weight,
    short_bias,
    embed_weight,
    embed_bias,
    inner_weight,
    inner_bias,
    filter_freq,
    filter_weight,
    filter_skip,
    output_gain,
    output_weight,
):
    row_count = lax.axis_size("row")
    row_index = lax.axis_index("row")
    col_index = lax.axis_index("col")
    local_tokens = tokens.shape[0]
    length = local_tokens * row_count
    col_width = first_gate.shape[1]
    own_width = col_width // row_count
    widened = tokens.astype(jnp.float32)
    normed = (
        widened
        * lax.rsqrt(jnp.mean(widened * widened, axis=1, keepdims=True) + NORM_EPS)
        * norm_gain
    ).astype(jnp.bfloat16)
    gate_first = jnp.dot(normed, first_gate, preferred_element_type=jnp.float32).astype(
        jnp.bfloat16
    )
    gate_second = jnp.dot(normed, second_gate, preferred_element_type=jnp.float32).astype(
        jnp.bfloat16
    )
    gate_value = jnp.dot(normed, value_weight, preferred_element_type=jnp.float32).astype(
        jnp.bfloat16
    )
    position_ramp, hidden = filter_hidden(
        length, embed_weight, embed_bias, inner_weight, inner_bias, filter_freq
    )
    channel_start = (col_index * row_count + row_index) * own_width
    deltas = lax.dynamic_slice_in_dim(decay_rates(), channel_start, own_width)
    tap_pairs = channel_taps(hidden, position_ramp, filter_weight, deltas)
    tables = make_tables(2 * length)
    half_width = short_weight.shape[1] // 2
    moved = (
        lax.all_to_all(gate_first, "row", split_axis=1, concat_axis=0, tiled=True),
        lax.all_to_all(gate_second, "row", split_axis=1, concat_axis=0, tiled=True),
        lax.all_to_all(gate_value, "row", split_axis=1, concat_axis=0, tiled=True),
    )
    weights_own = lax.dynamic_slice_in_dim(short_weight, row_index * own_width, own_width, 2)
    bias_own = lax.dynamic_slice_in_dim(short_bias, row_index * own_width, own_width, 1)
    smoothed = [
        short_filter(
            jnp.pad(moved[branch], ((half_width, half_width), (0, 0))),
            weights_own[branch],
            bias_own[branch],
            length,
        )
        for branch in range(3)
    ]
    signal = smoothed[2]
    for order_index in range(2):
        signal = smoothed[order_index] * two_sided(
            signal,
            tap_pairs[order_index][0],
            tap_pairs[order_index][1],
            filter_skip[order_index],
            tables,
        )
    result = jax.tree.map(
        lambda part, own: part.astype(own.dtype),
        lax.all_to_all(for_sending(signal), "row", split_axis=0, concat_axis=1, tiled=True),
        signal,
    )
    group_width = CHANNELS // GROUPS
    grouped = result.reshape(local_tokens, col_width // group_width, group_width)
    scaled = grouped * lax.rsqrt(jnp.mean(grouped * grouped, axis=2, keepdims=True) + NORM_EPS)
    mix_local = (scaled.reshape(local_tokens, col_width) * output_gain).astype(jnp.bfloat16)
    gathered = lax.all_to_all(mix_local, "col", split_axis=0, concat_axis=1, tiled=True)
    return jnp.dot(gathered, output_weight, preferred_element_type=jnp.float32).astype(jnp.bfloat16)


LANES = 128
SUBLANES = 16
BF16 = jnp.bfloat16
F32 = jnp.float32


def fast_tables(length, rows, tile_rows, own):
    total = 2 * length
    majors = length // LANES
    n1 = (np.arange(rows)[None, :] * tile_rows + np.arange(tile_rows)[:, None]).reshape(-1)
    k1 = np.arange(majors) + 0.5
    angle = 2.0 * np.pi * np.outer(k1, n1) / (2 * majors)
    eye = np.eye(own)
    inner = np.concatenate([np.kron(np.cos(angle), eye), np.kron(-np.sin(angle), eye)], 0)
    inner_back = inner.T * (2.0 / total)
    n2 = np.arange(LANES)
    turn = np.repeat(2.0 * np.pi * np.outer(k1, n2) / total, own, axis=0)
    twiddle = np.stack([np.cos(turn), np.sin(turn)])
    phase = 2.0 * np.pi * (np.outer(n2, n2) % LANES) / LANES
    c, s = np.cos(phase), np.sin(phase)
    outer = np.block([[c, -s], [s, c]])
    ramp = np.linspace(0.0, 1.0, length)
    angles = 2.0 * np.pi * np.arange(length) / length
    bands = np.linspace(0.0001, FREQ_BANDS - 1, FREQ_BANDS)[:, None]
    feats = np.concatenate([ramp[None], np.cos(bands * angles), -np.sin(bands * angles)], 0)
    feats = np.pad(feats, ((0, -feats.shape[0] % SUBLANES), (0, 0))).astype(np.float32)
    high = feats.astype(BF16)
    low = (feats - high.astype(np.float32)).astype(BF16)
    return (
        jnp.asarray(inner, BF16),
        jnp.asarray(inner_back, BF16),
        jnp.asarray(twiddle, F32),
        jnp.asarray(outer, BF16),
        jnp.asarray(outer.T, BF16),
        jnp.asarray(np.concatenate([high, low, high], 0)),
    )


def bounded_sin(x):
    turns = jnp.round(x * (1.0 / math.pi))
    r = x - turns * 3.140625
    r = r - turns * 9.67502593994140625e-4
    r = r - turns * 1.509957990978376432e-7
    half = turns * 0.5
    sign = 1.0 - 4.0 * (half - jnp.floor(half))
    q = r * r
    p = -2.5052108385e-8 + q * 1.6059043837e-10
    p = 2.7557319224e-6 + q * p
    p = -1.9841269841e-4 + q * p
    p = 8.3333333333e-3 + q * p
    p = -1.6666666667e-1 + q * p
    return sign * (r + r * q * p)


def mm(a, b):
    return jnp.dot(a.astype(BF16), b.astype(BF16), preferred_element_type=F32)


def halves(x):
    high = x.astype(BF16).astype(F32)
    return high, x - high


def tdot(a, stacked):
    high, low = halves(a)
    return lax.dot_general(
        jnp.concatenate([high, high, low], 0).astype(BF16),
        stacked,
        (((0,), (0,)), ((), ())),
        preferred_element_type=F32,
    )


def stack(b):
    high, low = halves(b)
    return jnp.concatenate([high, low, high], 0).astype(BF16)


def column(row, start, count):
    shape = (count, row.shape[1])
    hit = lax.broadcasted_iota(jnp.int32, shape, 1) == start + lax.broadcasted_iota(
        jnp.int32, shape, 0
    )
    return jnp.sum(jnp.where(hit, row.astype(F32), 0.0), axis=1, keepdims=True)


SMALL = 11


def fast_kernel(dims, *refs):
    tokens_h, first_h, second_h, value_h, out_w_h = refs[:5]
    small_h = refs[5 : 5 + SMALL]
    inner_h, inner_back_h, twiddle_h, outer_h, outer_back_h, feats_h, out_ref = refs[
        5 + SMALL : 12 + SMALL
    ]
    tokens_v, gates_v, out_w_v = refs[12 + SMALL : 15 + SMALL]
    small_v = refs[15 + SMALL : 15 + 2 * SMALL]
    (
        norm_gain, short_weight, short_bias, embed_weight, embed_bias, inner_weight,
        inner_bias, filter_freq, filter_weight, filter_skip, output_gain,
    ) = small_v
    (
        inner_v, inner_back_v, twiddle_v, outer_v, outer_back_v, feats_v, normed_v,
        send_a, recv_a, send_b, recv_b, send_s, recv_s, second_v, send_h, recv_h, gains,
        gain_map, spectra, embed_pad, load_sem, small_sem, send_a_sem, recv_a_sem, send_b_sem,
        recv_b_sem, send_g_sem, recv_g_sem, send_s_sem, recv_s_sem, send_h_sem, recv_h_sem,
    ) = refs[15 + 2 * SMALL :]
    rows_n, cols_n, block, own = dims
    length = rows_n * block
    tiles = block // LANES
    piece = block // cols_n
    groups = LANES // piece
    half = own // groups
    row_me = lax.axis_index("row")
    col_me = lax.axis_index("col")
    me = row_me * cols_n + col_me
    everyone = rows_n * cols_n

    loads = [
        (tokens_h, tokens_v),
        (value_h, gates_v.at[2]),
        (second_h, gates_v.at[1]),
        (first_h, gates_v.at[0]),
        (feats_h, feats_v),
        (inner_h, inner_v),
        (twiddle_h, twiddle_v),
        (outer_h, outer_v),
        (outer_back_h, outer_back_v),
        (inner_back_h, inner_back_v),
    ] + [(out_w_h.at[:, g], out_w_v.at[g]) for g in range(groups)]
    copies = [
        pltpu.make_async_copy(src, dst, load_sem.at[i]) for i, (src, dst) in enumerate(loads)
    ]
    smalls = [
        pltpu.make_async_copy(src, dst, small_sem.at[i])
        for i, (src, dst) in enumerate(zip(small_h, small_v))
    ]
    copies[0].start()
    smalls[0].start()
    copies[1].start()

    def place(flat):
        return (lax.div(flat, cols_n), lax.rem(flat, cols_n))

    barrier = pltpu.get_barrier_semaphore()
    for step in range(1, everyone):
        pl.semaphore_signal(
            barrier,
            inc=1,
            device_id=place(lax.rem(me + step, everyone)),
            device_id_type=pl.DeviceIdType.MESH,
        )

    for copy in copies[2:10] + smalls[1:]:
        copy.start()
    copies[0].wait()
    smalls[0].wait()
    gain_row = norm_gain[...]
    chunk = 32
    for start in range(0, block, chunk):
        x = tokens_v[start : start + chunk, :].astype(F32)
        scale = lax.rsqrt(jnp.mean(x * x, axis=1, keepdims=True) + NORM_EPS)
        normed_v[start : start + chunk, :] = (x * scale * gain_row).astype(BF16)

    MESH = pl.DeviceIdType.MESH
    sends = []

    def project(order, branch):
        copies[1 + 2 * order].wait()
        gate = jnp.dot(normed_v[...], gates_v[branch], preferred_element_type=F32)
        send_a[order] = gate.T.astype(BF16).reshape(rows_n, own, block)
        if order == 0:
            pl.semaphore_wait(barrier, everyone - 1)
        for step in range(1, rows_n):
            peer = lax.rem(row_me + step, rows_n)
            copy = pltpu.make_async_remote_copy(
                src_ref=send_a.at[order, peer],
                dst_ref=recv_a.at[order, row_me],
                send_sem=send_a_sem.at[order, step],
                recv_sem=recv_a_sem.at[order, step],
                device_id=(peer, col_me),
                device_id_type=MESH,
            )
            copy.start()
            sends.append((order, copy))
        recv_a[order, row_me] = send_a[order, row_me]

    project(0, 2)
    copies[2].wait()
    gate = jnp.dot(normed_v[...], gates_v[1], preferred_element_type=F32)
    gate = gate.astype(BF16).astype(F32)
    second_v[...] = gate.T
    send_h[0] = gate[:1]
    send_h[1] = gate[block - 1 :]
    halo_sends = []
    for edge, shift in ((0, rows_n - 1), (1, 1)):
        copy = pltpu.make_async_remote_copy(
            src_ref=send_h.at[edge],
            dst_ref=recv_h.at[edge],
            send_sem=send_h_sem.at[edge],
            recv_sem=recv_h_sem.at[edge],
            device_id=(lax.rem(row_me + shift, rows_n), col_me),
            device_id_type=MESH,
        )
        copy.start()
        halo_sends.append(copy)
    project(1, 0)
    for copy in copies[10:]:
        copy.start()
    for copy in smalls[1:]:
        copy.wait()

    gain_sends = []
    gains[col_me] = output_gain[...]
    for step in range(1, cols_n):
        copy = pltpu.make_async_remote_copy(
            src_ref=output_gain,
            dst_ref=gains.at[col_me],
            send_sem=send_g_sem.at[step],
            recv_sem=recv_g_sem.at[step],
            device_id=(row_me, lax.rem(col_me + step, cols_n)),
            device_id_type=pl.DeviceIdType.MESH,
        )
        copy.start()
        gain_sends.append(copy)

    def to_layout(x):
        return jnp.concatenate(
            [
                jnp.concatenate(
                    [
                        x[:, g * half : (g + 1) * half, j * LANES : (j + 1) * LANES].reshape(
                            rows_n * half, LANES
                        )
                        for g in range(groups)
                    ],
                    axis=1,
                )
                for j in range(tiles)
            ],
            axis=0,
        )

    def taps_layout(x):
        return jnp.concatenate(
            [
                jnp.concatenate(
                    [
                        x[
                            g * half : (g + 1) * half,
                            (r * tiles + j) * LANES : (r * tiles + j + 1) * LANES,
                        ]
                        for g in range(groups)
                    ],
                    axis=1,
                )
                for j in range(tiles)
                for r in range(rows_n)
            ],
            axis=0,
        )

    freq = column(filter_freq[...], 0, filter_freq.shape[1])
    copies[4].wait()
    embed_pad[...] = jnp.zeros_like(embed_pad)
    embed_pad[: embed_weight.shape[0], :] = embed_weight[...]
    hidden = bounded_sin(
        freq
        * (
            tdot(embed_pad[...], feats_v[...])
            + column(embed_bias[...], 0, embed_bias.shape[1])
        )
    )
    hidden = bounded_sin(
        freq * (tdot(inner_weight[...], stack(hidden)) + column(inner_bias[...], 0, inner_bias.shape[1]))
    )
    channels = rows_n * cols_n * own
    slowest = math.log(DECAY_TARGET) / SLOW_SPAN
    fastest = math.log(DECAY_TARGET) / FAST_SPAN
    channel = (
        (col_me * rows_n + row_me) * own + lax.broadcasted_iota(jnp.int32, (own, 1), 0)
    ).astype(F32)
    decay = jnp.abs(slowest + channel * ((fastest - slowest) / (channels - 1)))
    lag = lax.broadcasted_iota(jnp.int32, (own, length), 1)
    window = jnp.exp(-(lag.astype(F32) * (1.0 / (length - 1))) * decay)
    for copy in copies[5:8]:
        copy.wait()

    def twist(real, imag, sign):
        cos = jnp.concatenate([twiddle_v[0]] * groups, axis=1)
        sin = jnp.concatenate([twiddle_v[1]] * groups, axis=1) * sign
        return real * cos + imag * sin, imag * cos - real * sin

    def lanes_of(x, g):
        return x[:, g * LANES : (g + 1) * LANES]

    def forward_inner(x):
        part = mm(inner_v[...], x)
        count = part.shape[0] // 2
        return twist(part[:count], part[count:], 1.0)

    high, low = halves(filter_weight[...].reshape(4 * own, filter_weight.shape[3]))
    taps = jnp.dot(
        jnp.concatenate([high, high, low], 1).astype(BF16),
        stack(hidden),
        preferred_element_type=F32,
    )
    for order in range(2):
        fwd = taps[2 * order * own : (2 * order + 1) * own] * window
        bwd = taps[(2 * order + 1) * own : (2 * order + 2) * own] * window
        bwd = jnp.where(lag == 0, 0.0, bwd)
        plus = forward_inner(taps_layout(fwd + bwd))
        minus = forward_inner(taps_layout(fwd - bwd))
        for g in range(groups):
            p = jnp.concatenate([lanes_of(plus[0], g), lanes_of(plus[1], g)], axis=1)
            m = jnp.concatenate([lanes_of(minus[0], g), lanes_of(minus[1], g)], axis=1)
            spectra[order, g, :, :LANES] = mm(p, outer_v[:, :LANES])
            spectra[order, g, :, LANES:] = mm(m, outer_v[:, LANES:])

    for copy in halo_sends:
        copy.wait_recv()
    width = rows_n * own
    count = rows_n * half
    x = second_v[...]
    spot = lax.broadcasted_iota(jnp.int32, (width, block), 1)
    first_col = jnp.where(row_me == 0, 0.0, column(recv_h[1], 0, width))
    last_col = jnp.where(row_me == rows_n - 1, 0.0, column(recv_h[0], 0, width))
    before = jnp.where(spot == 0, first_col, pltpu.roll(x, 1, 1))
    after = jnp.where(spot == block - 1, last_col, pltpu.roll(x, block - 1, 1))
    w = [column(short_weight[1, j : j + 1, :], 0, width) for j in range(3)]
    x = column(short_bias[1:2, :], 0, width) + before * w[0] + x * w[1] + after * w[2]
    x = x.reshape(rows_n, groups, half, block)
    for q in range(cols_n):
        part = jnp.concatenate(
            [x[:, g, :, q * piece : (q + 1) * piece].reshape(count, piece) for g in range(groups)],
            axis=1,
        )
        send_s[q] = part.astype(BF16)
    recv_s[col_me] = send_s[col_me]
    second_sends = []
    for step in range(1, cols_n):
        peer = lax.rem(col_me + step, cols_n)
        copy = pltpu.make_async_remote_copy(
            src_ref=send_s.at[peer],
            dst_ref=recv_s.at[col_me],
            send_sem=send_s_sem.at[step],
            recv_sem=recv_s_sem.at[step],
            device_id=(row_me, peer),
            device_id_type=MESH,
        )
        copy.start()
        second_sends.append(copy)

    for copy in copies[8:10]:
        copy.wait()
    pos = lax.broadcasted_iota(jnp.int32, (rows_n, own, block), 2)

    def smooth(slot, branch):
        for b, copy in sends:
            if b == slot:
                copy.wait_recv()
        x = recv_a[slot].astype(F32)
        flat = x.reshape(rows_n * own, block)
        before = pltpu.roll(flat, 1, 1).reshape(rows_n, own, block)
        after = pltpu.roll(flat, block - 1, 1).reshape(rows_n, own, block)
        gap = jnp.zeros((1, own, block), F32)
        before = jnp.where(pos == 0, jnp.concatenate([gap, before[:-1]], 0), before)
        after = jnp.where(pos == block - 1, jnp.concatenate([after[1:], gap], 0), after)
        start = row_me * own
        w = [
            column(short_weight[branch, j : j + 1, :], start, own).reshape(1, own, 1)
            for j in range(3)
        ]
        bias = column(short_bias[branch : branch + 1, :], start, own).reshape(1, own, 1)
        return to_layout(bias + before * w[0] + x * w[1] + after * w[2])

    signal = smooth(0, 2)
    for order in range(2):
        real, imag = forward_inner(signal)
        back_real, back_imag = [], []
        for g in range(groups):
            t = jnp.concatenate([lanes_of(real, g), lanes_of(imag, g)], axis=1)
            spec = mm(t, outer_v[...])
            sr, si = spec[:, :LANES], spec[:, LANES:]
            hr, hi = spectra[order, g, :, :LANES], spectra[order, g, :, LANES:]
            prod = jnp.concatenate([sr * hr - si * hi, sr * hi + si * hr], axis=1)
            back = mm(prod, outer_back_v[...])
            back_real.append(back[:, :LANES])
            back_imag.append(back[:, LANES:])
        ur, ui = twist(jnp.concatenate(back_real, 1), jnp.concatenate(back_imag, 1), -1.0)
        conv = mm(inner_back_v[...], jnp.concatenate([ur, ui], axis=0))
        skip = column(filter_skip[order : order + 1, :], 0, own)
        skip = to_layout(jnp.broadcast_to(skip[None], (rows_n, own, block)))
        signal = conv + signal * skip
        if order == 0:
            signal = signal * smooth(1, 0)

    for j in range(tiles):
        for h in range(LANES // piece):
            part = jnp.concatenate(
                [
                    signal[
                        j * count : (j + 1) * count,
                        g * LANES + h * piece : g * LANES + (h + 1) * piece,
                    ]
                    for g in range(groups)
                ],
                axis=1,
            )
            send_b[j * (LANES // piece) + h] = part.astype(BF16).reshape(rows_n, half, LANES)
    last = []
    for step in sorted(range(1, everyone), key=lambda d: -min(d, everyone - d)):
        row_to, col_to = place(lax.rem(me + step, everyone))
        copy = pltpu.make_async_remote_copy(
            src_ref=send_b.at[col_to, row_to],
            dst_ref=recv_b.at[col_me, row_me],
            send_sem=send_b_sem.at[step],
            recv_sem=recv_b_sem.at[step],
            device_id=(row_to, col_to),
            device_id_type=pl.DeviceIdType.MESH,
        )
        copy.start()
        last.append(copy)
    recv_b[col_me, row_me] = send_b[col_me, row_me]

    for copy in gain_sends:
        copy.wait_recv()
    lane = lax.broadcasted_iota(jnp.int32, (rows_n * half, LANES), 1)
    for q in range(cols_n):
        col_gain = column(gains[q], 0, width).reshape(rows_n, own, 1)
        result = jnp.zeros((rows_n * half, LANES), F32)
        for g in range(groups):
            part = col_gain[:, g * half : (g + 1) * half].reshape(rows_n * half, 1)
            result = jnp.where(lax.div(lane, piece) == g, part, result)
        gain_map[q] = result
    for copy in copies[10:]:
        copy.wait()
    for copy in second_sends + last:
        copy.wait_recv()

    group_width = CHANNELS // GROUPS
    per_group = group_width // own
    turned = []
    for q in range(cols_n):
        for r in range(0, rows_n, per_group):
            x = recv_b[q, r : r + per_group].astype(F32).reshape(per_group * half, LANES)
            x = x * recv_s[q, r * half : (r + per_group) * half, :].astype(F32)
            total = jnp.sum(x * x, axis=0, keepdims=True)
            square = total
            for g in range(1, groups):
                square = square + pltpu.roll(total, g * piece, 1)
            scale = lax.rsqrt(square * (1.0 / group_width) + NORM_EPS)
            gain = gain_map[q, r * half : (r + per_group) * half, :]
            turned.append(x * scale * gain)
    mixed = jnp.concatenate(turned, axis=0).T.astype(BF16)
    depth = everyone * half
    step_width = 512
    for start in range(0, out_ref.shape[1], step_width):
        acc = jnp.zeros((piece, step_width), F32)
        for g in range(groups):
            acc = acc + jnp.dot(
                mixed[g * piece : (g + 1) * piece],
                out_w_v[g, :, :, start : start + step_width].reshape(depth, step_width),
                preferred_element_type=F32,
            )
        out_ref[:, start : start + step_width] = acc.astype(BF16)

    for _, copy in sends:
        copy.wait_send()
    for copy in halo_sends + gain_sends + second_sends + last:
        copy.wait_send()


def fast_local(*args):
    (
        tokens, norm_gain, first_gate, second_gate, value_weight, short_weight, short_bias,
        embed_weight, embed_bias, inner_weight, inner_bias, filter_freq, filter_weight,
        filter_skip, output_gain, output_weight,
    ) = args
    rows_n, cols_n = lax.axis_size("row"), lax.axis_size("col")
    block, model = tokens.shape
    own = filter_weight.shape[3]
    piece = block // cols_n
    groups = LANES // piece
    half = own // groups
    tiles = block // LANES
    length = block * rows_n
    width = first_gate.shape[1]
    everyone = rows_n * cols_n
    tables = fast_tables(length, rows_n, tiles, half)
    out_width = output_weight.shape[1]
    out_w = output_weight.reshape(everyone, groups, half, out_width)
    vm = pl.BlockSpec(memory_space=pltpu.VMEM)
    hbm = pl.BlockSpec(memory_space=pl.ANY)
    small = [
        norm_gain.reshape(1, -1),
        short_weight,
        short_bias,
        embed_weight,
        embed_bias.reshape(1, -1),
        inner_weight,
        inner_bias.reshape(1, -1),
        filter_freq.reshape(1, -1),
        jnp.swapaxes(filter_weight, 2, 3),
        filter_skip,
        output_gain.reshape(1, -1),
    ]
    operands = [tokens, first_gate, second_gate, value_weight, out_w, *small, *tables]
    rows_all = tiles * rows_n * half
    DMA = pltpu.SemaphoreType.DMA
    return pl.pallas_call(
        functools.partial(fast_kernel, (rows_n, cols_n, block, own)),
        out_shape=pltpu.VMEM((piece, out_width), BF16),
        in_specs=[hbm] * len(operands),
        out_specs=vm,
        scratch_shapes=[
            pltpu.VMEM(tokens.shape, BF16),
            pltpu.VMEM((3, model, width), BF16),
            pltpu.VMEM((groups, everyone, half, out_width), BF16),
        ]
        + [pltpu.VMEM(array.shape, array.dtype) for array in small + list(tables)]
        + [
            pltpu.VMEM(tokens.shape, BF16),
            pltpu.VMEM((2, rows_n, own, block), BF16),
            pltpu.VMEM((2, rows_n, own, block), BF16),
            pltpu.VMEM((cols_n, rows_n, half, LANES), BF16),
            pltpu.VMEM((cols_n, rows_n, half, LANES), BF16),
            pltpu.VMEM((cols_n, rows_n * half, LANES), BF16),
            pltpu.VMEM((cols_n, rows_n * half, LANES), BF16),
            pltpu.VMEM((width, block), F32),
            pltpu.VMEM((2, 1, width), F32),
            pltpu.VMEM((2, 1, width), F32),
            pltpu.VMEM((cols_n, 1, width), F32),
            pltpu.VMEM((cols_n, rows_n * half, LANES), F32),
            pltpu.VMEM((2, groups, rows_all, 2 * LANES), F32),
            pltpu.VMEM((tables[-1].shape[0] // 3, embed_weight.shape[1]), F32),
            DMA((10 + groups,)),
            DMA((SMALL,)),
            DMA((2, rows_n)),
            DMA((2, rows_n)),
            DMA((everyone,)),
            DMA((everyone,)),
            DMA((cols_n,)),
            DMA((cols_n,)),
            DMA((cols_n,)),
            DMA((cols_n,)),
            DMA((2,)),
            DMA((2,)),
        ],
        compiler_params=pltpu.CompilerParams(
            collective_id=0, has_side_effects=True, vmem_limit_bytes=56 * 1024 * 1024
        ),
    )(*operands)


def kernel_fits(tokens, filter_weight, rows_n, cols_n):
    block = tokens.shape[0]
    own = filter_weight.shape[3]
    piece = block // cols_n
    if block % LANES or LANES % piece:
        return False
    groups = LANES // piece
    return own % (groups * SUBLANES) == 0 and (CHANNELS // GROUPS) % own == 0


def local(*args):
    if kernel_fits(args[0], args[12], lax.axis_size("row"), lax.axis_size("col")):
        return fast_local(*args)
    return general_local(*args)


def solution(mesh):
    in_specs = (
        P("row", None),
        P(),
        P(None, "col"),
        P(None, "col"),
        P(None, "col"),
        P(None, None, "col"),
        P(None, "col"),
        P(),
        P(),
        P(),
        P(),
        P(),
        P(None, None, None, ("col", "row")),
        P(None, ("col", "row")),
        P("col"),
        P(),
    )
    out_specs = P(("row", "col"), None)
    return jax.shard_map(local, mesh=mesh, in_specs=in_specs, out_specs=out_specs, check_vma=False)
```

```python
import functools
import math

import jax
import jax.numpy as jnp
import numpy as np
from jax import lax
from jax.experimental import pallas as pl
from jax.experimental.pallas import tpu as pltpu
from jax.sharding import PartitionSpec as P

CHANNELS = 1024
GROUPS = 8
FREQ_BANDS = 16


HIGHEST = lax.Precision.HIGHEST
NORM_EPS = 1e-06
DECAY_TARGET = 0.01
FAST_SPAN = 0.3
SLOW_SPAN = 1.5


def for_sending(value):
    return jax.tree.map(lambda a: a.astype(jnp.bfloat16) if a.dtype == jnp.float32 else a, value)


def position_features(length):
    position_ramp = jnp.linspace(0.0, 1.0, length, dtype=jnp.float32)[:, None]
    angles = 2.0 * math.pi * jnp.arange(length, dtype=jnp.float32)[:, None] / length
    band_freqs = jnp.linspace(0.0001, FREQ_BANDS - 1, FREQ_BANDS, dtype=jnp.float32)[None, :]
    features = jnp.concatenate(
        [position_ramp, jnp.cos(band_freqs * angles), -jnp.sin(band_freqs * angles)], axis=1
    )
    return (position_ramp, features)


def filter_hidden(length, embed_weight, embed_bias, inner_weight, inner_bias, filter_freq):
    position_ramp, features = position_features(length)
    hidden = jnp.sin(
        filter_freq * (jnp.dot(features, embed_weight, precision=HIGHEST) + embed_bias)
    )
    hidden = jnp.sin(filter_freq * (jnp.dot(hidden, inner_weight, precision=HIGHEST) + inner_bias))
    return (position_ramp, hidden)


def decay_rates():
    fastest = math.log(DECAY_TARGET) / FAST_SPAN
    slowest = math.log(DECAY_TARGET) / SLOW_SPAN
    return jnp.abs(jnp.linspace(slowest, fastest, CHANNELS, dtype=jnp.float32))


def short_filter(padded, weights, bias_row, length):
    result = bias_row.astype(jnp.float32)
    for tap_index in range(weights.shape[0]):
        result = result + padded[tap_index : tap_index + length].astype(jnp.float32) * weights[
            tap_index
        ].astype(jnp.float32)
    return result


def phase_table(rows, cols, period):
    phase_index = (
        lax.broadcasted_iota(jnp.int32, (rows, cols), 0)
        * lax.broadcasted_iota(jnp.int32, (rows, cols), 1)
        % period
    )
    phase_angle = phase_index.astype(jnp.float32) * (2.0 * math.pi / period)
    return (jnp.cos(phase_angle), jnp.sin(phase_angle))


def split_length(total_size):
    chosen = 2
    for candidate in range(2, math.isqrt(total_size) + 1, 2):
        if total_size % candidate == 0:
            chosen = candidate
    return chosen


def make_tables(total_size):
    major_size = split_length(total_size)
    minor_size = total_size // major_size
    inner_table = phase_table(major_size, major_size, major_size)
    twiddle = phase_table(major_size, minor_size, total_size)
    outer_table = phase_table(minor_size, minor_size, minor_size)
    return (major_size, minor_size, inner_table, twiddle, outer_table)


def finish_forward(part_real, part_imag, twiddle, outer_table):
    turn_cos = twiddle[0][:, :, None]
    turn_sin = twiddle[1][:, :, None]
    turned_real = part_real * turn_cos + part_imag * turn_sin
    turned_imag = part_imag * turn_cos - part_real * turn_sin
    outer_cos, outer_sin = outer_table
    spec_real = jnp.einsum("anc,nk->akc", turned_real, outer_cos, precision=HIGHEST) + jnp.einsum(
        "anc,nk->akc", turned_imag, outer_sin, precision=HIGHEST
    )
    spec_imag = jnp.einsum("anc,nk->akc", turned_imag, outer_cos, precision=HIGHEST) - jnp.einsum(
        "anc,nk->akc", turned_real, outer_sin, precision=HIGHEST
    )
    return (spec_real, spec_imag)


def forward_signal(signal, tables):
    major_size, minor_size, inner_table, twiddle, outer_table = tables
    channels = signal.shape[1]
    flattened = signal.reshape(major_size // 2, minor_size * channels)
    inner_cos = inner_table[0][:, : major_size // 2]
    inner_sin = inner_table[1][:, : major_size // 2]
    part_real = jnp.dot(inner_cos, flattened, precision=HIGHEST).reshape(
        major_size, minor_size, channels
    )
    part_imag = -jnp.dot(inner_sin, flattened, precision=HIGHEST).reshape(
        major_size, minor_size, channels
    )
    return finish_forward(part_real, part_imag, twiddle, outer_table)


def forward_taps(circular_taps, tables):
    major_size, minor_size, inner_table, twiddle, outer_table = tables
    channels = circular_taps.shape[1]
    flattened = circular_taps.reshape(major_size, minor_size * channels)
    part_real = jnp.dot(inner_table[0], flattened, precision=HIGHEST).reshape(
        major_size, minor_size, channels
    )
    part_imag = -jnp.dot(inner_table[1], flattened, precision=HIGHEST).reshape(
        major_size, minor_size, channels
    )
    return finish_forward(part_real, part_imag, twiddle, outer_table)


def inverse(spec_real, spec_imag, tables):
    major_size, minor_size, inner_table, twiddle, outer_table = tables
    channels = spec_real.shape[2]
    outer_cos, outer_sin = outer_table
    back_real = jnp.einsum("akc,kn->anc", spec_real, outer_cos, precision=HIGHEST) - jnp.einsum(
        "akc,kn->anc", spec_imag, outer_sin, precision=HIGHEST
    )
    back_imag = jnp.einsum("akc,kn->anc", spec_imag, outer_cos, precision=HIGHEST) + jnp.einsum(
        "akc,kn->anc", spec_real, outer_sin, precision=HIGHEST
    )
    turn_cos = twiddle[0][:, :, None]
    turn_sin = twiddle[1][:, :, None]
    turned_real = (back_real * turn_cos - back_imag * turn_sin).reshape(
        major_size, minor_size * channels
    )
    turned_imag = (back_imag * turn_cos + back_real * turn_sin).reshape(
        major_size, minor_size * channels
    )
    half_rows = major_size // 2
    values = jnp.dot(inner_table[0][:half_rows], turned_real, precision=HIGHEST) - jnp.dot(
        inner_table[1][:half_rows], turned_imag, precision=HIGHEST
    )
    return values.reshape(half_rows * minor_size, channels) / (major_size * minor_size)


def two_sided(signal, forward, backward, skip_gain, tables):
    circular_taps = jnp.concatenate([forward, jnp.zeros_like(forward[:1]), backward[:0:-1]], axis=0)
    signal_real, signal_imag = forward_signal(signal, tables)
    taps_real, taps_imag = forward_taps(circular_taps, tables)
    prod_real = signal_real * taps_real - signal_imag * taps_imag
    prod_imag = signal_real * taps_imag + signal_imag * taps_real
    return inverse(prod_real, prod_imag, tables) + signal * skip_gain


def channel_taps(hidden, position_ramp, filter_weight, deltas):
    window = jnp.exp(-position_ramp * deltas[None, :])
    pairs = []
    for order_index in range(filter_weight.shape[0]):
        forward = jnp.dot(hidden, filter_weight[order_index, 0], precision=HIGHEST) * window
        backward = jnp.dot(hidden, filter_weight[order_index, 1], precision=HIGHEST) * window
        pairs.append((forward, backward))
    return pairs


def general_local(
    tokens,
    norm_gain,
    first_gate,
    second_gate,
    value_weight,
    short_weight,
    short_bias,
    embed_weight,
    embed_bias,
    inner_weight,
    inner_bias,
    filter_freq,
    filter_weight,
    filter_skip,
    output_gain,
    output_weight,
):
    row_count = lax.axis_size("row")
    row_index = lax.axis_index("row")
    col_index = lax.axis_index("col")
    local_tokens = tokens.shape[0]
    length = local_tokens * row_count
    col_width = first_gate.shape[1]
    own_width = col_width // row_count
    widened = tokens.astype(jnp.float32)
    normed = (
        widened
        * lax.rsqrt(jnp.mean(widened * widened, axis=1, keepdims=True) + NORM_EPS)
        * norm_gain
    ).astype(jnp.bfloat16)
    gate_first = jnp.dot(normed, first_gate, preferred_element_type=jnp.float32).astype(
        jnp.bfloat16
    )
    gate_second = jnp.dot(normed, second_gate, preferred_element_type=jnp.float32).astype(
        jnp.bfloat16
    )
    gate_value = jnp.dot(normed, value_weight, preferred_element_type=jnp.float32).astype(
        jnp.bfloat16
    )
    position_ramp, hidden = filter_hidden(
        length, embed_weight, embed_bias, inner_weight, inner_bias, filter_freq
    )
    channel_start = (col_index * row_count + row_index) * own_width
    deltas = lax.dynamic_slice_in_dim(decay_rates(), channel_start, own_width)
    tap_pairs = channel_taps(hidden, position_ramp, filter_weight, deltas)
    tables = make_tables(2 * length)
    half_width = short_weight.shape[1] // 2
    moved = (
        lax.all_to_all(gate_first, "row", split_axis=1, concat_axis=0, tiled=True),
        lax.all_to_all(gate_second, "row", split_axis=1, concat_axis=0, tiled=True),
        lax.all_to_all(gate_value, "row", split_axis=1, concat_axis=0, tiled=True),
    )
    weights_own = lax.dynamic_slice_in_dim(short_weight, row_index * own_width, own_width, 2)
    bias_own = lax.dynamic_slice_in_dim(short_bias, row_index * own_width, own_width, 1)
    smoothed = [
        short_filter(
            jnp.pad(moved[branch], ((half_width, half_width), (0, 0))),
            weights_own[branch],
            bias_own[branch],
            length,
        )
        for branch in range(3)
    ]
    signal = smoothed[2]
    for order_index in range(2):
        signal = smoothed[order_index] * two_sided(
            signal,
            tap_pairs[order_index][0],
            tap_pairs[order_index][1],
            filter_skip[order_index],
            tables,
        )
    result = jax.tree.map(
        lambda part, own: part.astype(own.dtype),
        lax.all_to_all(for_sending(signal), "row", split_axis=0, concat_axis=1, tiled=True),
        signal,
    )
    group_width = CHANNELS // GROUPS
    grouped = result.reshape(local_tokens, col_width // group_width, group_width)
    scaled = grouped * lax.rsqrt(jnp.mean(grouped * grouped, axis=2, keepdims=True) + NORM_EPS)
    mix_local = (scaled.reshape(local_tokens, col_width) * output_gain).astype(jnp.bfloat16)
    gathered = lax.all_to_all(mix_local, "col", split_axis=0, concat_axis=1, tiled=True)
    return jnp.dot(gathered, output_weight, preferred_element_type=jnp.float32).astype(jnp.bfloat16)


LANES = 128
SUBLANES = 16
BF16 = jnp.bfloat16
F32 = jnp.float32


def fast_tables(length, rows, tile_rows, own):
    total = 2 * length
    majors = length // LANES
    n1 = (np.arange(rows)[None, :] * tile_rows + np.arange(tile_rows)[:, None]).reshape(-1)
    k1 = np.arange(majors) + 0.5
    angle = 2.0 * np.pi * np.outer(k1, n1) / (2 * majors)
    eye = np.eye(own)
    inner = np.concatenate([np.kron(np.cos(angle), eye), np.kron(-np.sin(angle), eye)], 0)
    inner_back = inner.T * (2.0 / total)
    n2 = np.arange(LANES)
    turn = np.repeat(2.0 * np.pi * np.outer(k1, n2) / total, own, axis=0)
    twiddle = np.stack([np.cos(turn), np.sin(turn)])
    phase = 2.0 * np.pi * (np.outer(n2, n2) % LANES) / LANES
    c, s = np.cos(phase), np.sin(phase)
    outer = np.block([[c, -s], [s, c]])
    ramp = np.linspace(0.0, 1.0, length)
    angles = 2.0 * np.pi * np.arange(length) / length
    bands = np.linspace(0.0001, FREQ_BANDS - 1, FREQ_BANDS)[:, None]
    feats = np.concatenate([ramp[None], np.cos(bands * angles), -np.sin(bands * angles)], 0)
    feats = np.pad(feats, ((0, -feats.shape[0] % SUBLANES), (0, 0))).astype(np.float32)
    high = feats.astype(BF16)
    low = (feats - high.astype(np.float32)).astype(BF16)
    return (
        jnp.asarray(inner, BF16),
        jnp.asarray(inner_back, BF16),
        jnp.asarray(twiddle, F32),
        jnp.asarray(outer, BF16),
        jnp.asarray(outer.T, BF16),
        jnp.asarray(np.concatenate([high, low, high], 0)),
    )


def bounded_sin(x):
    turns = jnp.round(x * (1.0 / math.pi))
    r = x - turns * 3.140625
    r = r - turns * 9.67502593994140625e-4
    r = r - turns * 1.509957990978376432e-7
    half = turns * 0.5
    sign = 1.0 - 4.0 * (half - jnp.floor(half))
    q = r * r
    p = -2.5052108385e-8 + q * 1.6059043837e-10
    p = 2.7557319224e-6 + q * p
    p = -1.9841269841e-4 + q * p
    p = 8.3333333333e-3 + q * p
    p = -1.6666666667e-1 + q * p
    return sign * (r + r * q * p)


def mm(a, b):
    return jnp.dot(a.astype(BF16), b.astype(BF16), preferred_element_type=F32)


def halves(x):
    high = x.astype(BF16).astype(F32)
    return high, x - high


def tdot(a, stacked):
    high, low = halves(a)
    return lax.dot_general(
        jnp.concatenate([high, high, low], 0).astype(BF16),
        stacked,
        (((0,), (0,)), ((), ())),
        preferred_element_type=F32,
    )


def stack(b):
    high, low = halves(b)
    return jnp.concatenate([high, low, high], 0).astype(BF16)


def column(row, start, count):
    shape = (count, row.shape[1])
    hit = lax.broadcasted_iota(jnp.int32, shape, 1) == start + lax.broadcasted_iota(
        jnp.int32, shape, 0
    )
    return jnp.sum(jnp.where(hit, row.astype(F32), 0.0), axis=1, keepdims=True)


SMALL = 11


def fast_kernel(dims, *refs):
    tokens_h, first_h, second_h, value_h, out_w_h = refs[:5]
    small_h = refs[5 : 5 + SMALL]
    inner_h, inner_back_h, twiddle_h, outer_h, outer_back_h, feats_h, out_ref = refs[
        5 + SMALL : 12 + SMALL
    ]
    tokens_v, gates_v, out_w_v = refs[12 + SMALL : 15 + SMALL]
    small_v = refs[15 + SMALL : 15 + 2 * SMALL]
    (
        norm_gain, short_weight, short_bias, embed_weight, embed_bias, inner_weight,
        inner_bias, filter_freq, filter_weight, filter_skip, output_gain,
    ) = small_v
    (
        inner_v, inner_back_v, twiddle_v, outer_v, outer_back_v, feats_v, normed_v,
        send_a, recv_a, send_b, recv_b, send_s, recv_s, second_v, send_h, recv_h, gains,
        gain_map, spectra, embed_pad, load_sem, small_sem, send_a_sem, recv_a_sem, send_b_sem,
        recv_b_sem, send_g_sem, recv_g_sem, send_s_sem, recv_s_sem, send_h_sem, recv_h_sem,
    ) = refs[15 + 2 * SMALL :]
    rows_n, cols_n, block, own = dims
    length = rows_n * block
    tiles = block // LANES
    piece = block // cols_n
    groups = LANES // piece
    half = own // groups
    row_me = lax.axis_index("row")
    col_me = lax.axis_index("col")
    me = row_me * cols_n + col_me
    everyone = rows_n * cols_n

    loads = [
        (tokens_h, tokens_v),
        (value_h, gates_v.at[2]),
        (first_h, gates_v.at[0]),
        (second_h, gates_v.at[1]),
        (feats_h, feats_v),
        (inner_h, inner_v),
        (twiddle_h, twiddle_v),
        (outer_h, outer_v),
        (outer_back_h, outer_back_v),
        (inner_back_h, inner_back_v),
    ] + [(out_w_h.at[:, g], out_w_v.at[g]) for g in range(groups)]
    copies = [
        pltpu.make_async_copy(src, dst, load_sem.at[i]) for i, (src, dst) in enumerate(loads)
    ]
    smalls = [
        pltpu.make_async_copy(src, dst, small_sem.at[i])
        for i, (src, dst) in enumerate(zip(small_h, small_v))
    ]
    copies[0].start()
    smalls[0].start()
    copies[1].start()

    def place(flat):
        return (lax.div(flat, cols_n), lax.rem(flat, cols_n))

    barrier = pltpu.get_barrier_semaphore()
    for step in range(1, everyone):
        pl.semaphore_signal(
            barrier,
            inc=1,
            device_id=place(lax.rem(me + step, everyone)),
            device_id_type=pl.DeviceIdType.MESH,
        )

    for copy in copies[2:10] + smalls[1:]:
        copy.start()
    copies[0].wait()
    smalls[0].wait()
    gain_row = norm_gain[...]
    chunk = 32
    for start in range(0, block, chunk):
        x = tokens_v[start : start + chunk, :].astype(F32)
        scale = lax.rsqrt(jnp.mean(x * x, axis=1, keepdims=True) + NORM_EPS)
        normed_v[start : start + chunk, :] = (x * scale * gain_row).astype(BF16)

    MESH = pl.DeviceIdType.MESH
    sends = []

    def project(order, branch):
        copies[1 + order].wait()
        gate = jnp.dot(normed_v[...], gates_v[branch], preferred_element_type=F32)
        send_a[order] = gate.T.astype(BF16).reshape(rows_n, own, block)
        if order == 0:
            pl.semaphore_wait(barrier, everyone - 1)
        for step in range(1, rows_n):
            peer = lax.rem(row_me + step, rows_n)
            copy = pltpu.make_async_remote_copy(
                src_ref=send_a.at[order, peer],
                dst_ref=recv_a.at[order, row_me],
                send_sem=send_a_sem.at[order, step],
                recv_sem=recv_a_sem.at[order, step],
                device_id=(peer, col_me),
                device_id_type=MESH,
            )
            copy.start()
            sends.append((order, copy))
        recv_a[order, row_me] = send_a[order, row_me]

    project(0, 2)
    project(1, 0)
    copies[3].wait()
    gate = jnp.dot(normed_v[...], gates_v[1], preferred_element_type=F32)
    gate = gate.astype(BF16).astype(F32)
    second_v[...] = gate.T
    send_h[0] = gate[:1]
    send_h[1] = gate[block - 1 :]
    halo_sends = []
    for edge, shift in ((0, rows_n - 1), (1, 1)):
        copy = pltpu.make_async_remote_copy(
            src_ref=send_h.at[edge],
            dst_ref=recv_h.at[edge],
            send_sem=send_h_sem.at[edge],
            recv_sem=recv_h_sem.at[edge],
            device_id=(lax.rem(row_me + shift, rows_n), col_me),
            device_id_type=MESH,
        )
        copy.start()
        halo_sends.append(copy)
    for copy in copies[10:]:
        copy.start()
    for copy in smalls[1:]:
        copy.wait()

    gain_sends = []
    gains[col_me] = output_gain[...]
    for step in range(1, cols_n):
        copy = pltpu.make_async_remote_copy(
            src_ref=output_gain,
            dst_ref=gains.at[col_me],
            send_sem=send_g_sem.at[step],
            recv_sem=recv_g_sem.at[step],
            device_id=(row_me, lax.rem(col_me + step, cols_n)),
            device_id_type=pl.DeviceIdType.MESH,
        )
        copy.start()
        gain_sends.append(copy)

    def to_layout(x):
        return jnp.concatenate(
            [
                jnp.concatenate(
                    [
                        x[:, g * half : (g + 1) * half, j * LANES : (j + 1) * LANES].reshape(
                            rows_n * half, LANES
                        )
                        for g in range(groups)
                    ],
                    axis=1,
                )
                for j in range(tiles)
            ],
            axis=0,
        )

    def taps_layout(x):
        return jnp.concatenate(
            [
                jnp.concatenate(
                    [
                        x[
                            g * half : (g + 1) * half,
                            (r * tiles + j) * LANES : (r * tiles + j + 1) * LANES,
                        ]
                        for g in range(groups)
                    ],
                    axis=1,
                )
                for j in range(tiles)
                for r in range(rows_n)
            ],
            axis=0,
        )

    freq = column(filter_freq[...], 0, filter_freq.shape[1])
    copies[4].wait()
    embed_pad[...] = jnp.zeros_like(embed_pad)
    embed_pad[: embed_weight.shape[0], :] = embed_weight[...]
    hidden = bounded_sin(
        freq
        * (
            tdot(embed_pad[...], feats_v[...])
            + column(embed_bias[...], 0, embed_bias.shape[1])
        )
    )
    hidden = bounded_sin(
        freq * (tdot(inner_weight[...], stack(hidden)) + column(inner_bias[...], 0, inner_bias.shape[1]))
    )
    channels = rows_n * cols_n * own
    slowest = math.log(DECAY_TARGET) / SLOW_SPAN
    fastest = math.log(DECAY_TARGET) / FAST_SPAN
    channel = (
        (col_me * rows_n + row_me) * own + lax.broadcasted_iota(jnp.int32, (own, 1), 0)
    ).astype(F32)
    decay = jnp.abs(slowest + channel * ((fastest - slowest) / (channels - 1)))
    lag = lax.broadcasted_iota(jnp.int32, (own, length), 1)
    window = jnp.exp(-(lag.astype(F32) * (1.0 / (length - 1))) * decay)
    for copy in copies[5:8]:
        copy.wait()

    def twist(real, imag, sign):
        cos = jnp.concatenate([twiddle_v[0]] * groups, axis=1)
        sin = jnp.concatenate([twiddle_v[1]] * groups, axis=1) * sign
        return real * cos + imag * sin, imag * cos - real * sin

    def lanes_of(x, g):
        return x[:, g * LANES : (g + 1) * LANES]

    def forward_inner(x):
        part = mm(inner_v[...], x)
        count = part.shape[0] // 2
        return twist(part[:count], part[count:], 1.0)

    high, low = halves(filter_weight[...].reshape(4 * own, filter_weight.shape[3]))
    taps = jnp.dot(
        jnp.concatenate([high, high, low], 1).astype(BF16),
        stack(hidden),
        preferred_element_type=F32,
    )
    for order in range(2):
        fwd = taps[2 * order * own : (2 * order + 1) * own] * window
        bwd = taps[(2 * order + 1) * own : (2 * order + 2) * own] * window
        bwd = jnp.where(lag == 0, 0.0, bwd)
        plus = forward_inner(taps_layout(fwd + bwd))
        minus = forward_inner(taps_layout(fwd - bwd))
        for g in range(groups):
            p = jnp.concatenate([lanes_of(plus[0], g), lanes_of(plus[1], g)], axis=1)
            m = jnp.concatenate([lanes_of(minus[0], g), lanes_of(minus[1], g)], axis=1)
            spectra[order, g, :, :LANES] = mm(p, outer_v[:, :LANES])
            spectra[order, g, :, LANES:] = mm(m, outer_v[:, LANES:])

    width = rows_n * own
    count = rows_n * half
    second_sends = []

    def send_second():
        for copy in halo_sends:
            copy.wait_recv()
        x = second_v[...]
        spot = lax.broadcasted_iota(jnp.int32, (width, block), 1)
        first_col = jnp.where(row_me == 0, 0.0, column(recv_h[1], 0, width))
        last_col = jnp.where(row_me == rows_n - 1, 0.0, column(recv_h[0], 0, width))
        before = jnp.where(spot == 0, first_col, pltpu.roll(x, 1, 1))
        after = jnp.where(spot == block - 1, last_col, pltpu.roll(x, block - 1, 1))
        w = [column(short_weight[1, j : j + 1, :], 0, width) for j in range(3)]
        x = column(short_bias[1:2, :], 0, width) + before * w[0] + x * w[1] + after * w[2]
        x = x.reshape(rows_n, groups, half, block)
        for q in range(cols_n):
            part = jnp.concatenate(
                [x[:, g, :, q * piece : (q + 1) * piece].reshape(count, piece) for g in range(groups)],
                axis=1,
            )
            send_s[q] = part.astype(BF16)
        recv_s[col_me] = send_s[col_me]
        for step in range(1, cols_n):
            peer = lax.rem(col_me + step, cols_n)
            copy = pltpu.make_async_remote_copy(
                src_ref=send_s.at[peer],
                dst_ref=recv_s.at[col_me],
                send_sem=send_s_sem.at[step],
                recv_sem=recv_s_sem.at[step],
                device_id=(row_me, peer),
                device_id_type=MESH,
            )
            copy.start()
            second_sends.append(copy)

    for copy in copies[8:10]:
        copy.wait()
    pos = lax.broadcasted_iota(jnp.int32, (rows_n, own, block), 2)

    def smooth(slot, branch):
        for b, copy in sends:
            if b == slot:
                copy.wait_recv()
        x = recv_a[slot].astype(F32)
        flat = x.reshape(rows_n * own, block)
        before = pltpu.roll(flat, 1, 1).reshape(rows_n, own, block)
        after = pltpu.roll(flat, block - 1, 1).reshape(rows_n, own, block)
        gap = jnp.zeros((1, own, block), F32)
        before = jnp.where(pos == 0, jnp.concatenate([gap, before[:-1]], 0), before)
        after = jnp.where(pos == block - 1, jnp.concatenate([after[1:], gap], 0), after)
        start = row_me * own
        w = [
            column(short_weight[branch, j : j + 1, :], start, own).reshape(1, own, 1)
            for j in range(3)
        ]
        bias = column(short_bias[branch : branch + 1, :], start, own).reshape(1, own, 1)
        return to_layout(bias + before * w[0] + x * w[1] + after * w[2])

    signal = smooth(0, 2)
    for order in range(2):
        real, imag = forward_inner(signal)
        back_real, back_imag = [], []
        for g in range(groups):
            t = jnp.concatenate([lanes_of(real, g), lanes_of(imag, g)], axis=1)
            spec = mm(t, outer_v[...])
            sr, si = spec[:, :LANES], spec[:, LANES:]
            hr, hi = spectra[order, g, :, :LANES], spectra[order, g, :, LANES:]
            prod = jnp.concatenate([sr * hr - si * hi, sr * hi + si * hr], axis=1)
            back = mm(prod, outer_back_v[...])
            back_real.append(back[:, :LANES])
            back_imag.append(back[:, LANES:])
        ur, ui = twist(jnp.concatenate(back_real, 1), jnp.concatenate(back_imag, 1), -1.0)
        conv = mm(inner_back_v[...], jnp.concatenate([ur, ui], axis=0))
        skip = column(filter_skip[order : order + 1, :], 0, own)
        skip = to_layout(jnp.broadcast_to(skip[None], (rows_n, own, block)))
        signal = conv + signal * skip
        if order == 0:
            send_second()
            signal = signal * smooth(1, 0)

    for j in range(tiles):
        for h in range(LANES // piece):
            part = jnp.concatenate(
                [
                    signal[
                        j * count : (j + 1) * count,
                        g * LANES + h * piece : g * LANES + (h + 1) * piece,
                    ]
                    for g in range(groups)
                ],
                axis=1,
            )
            send_b[j * (LANES // piece) + h] = part.astype(BF16).reshape(rows_n, half, LANES)
    last = []
    for step in range(1, everyone):
        row_to, col_to = place(lax.rem(me + step, everyone))
        copy = pltpu.make_async_remote_copy(
            src_ref=send_b.at[col_to, row_to],
            dst_ref=recv_b.at[col_me, row_me],
            send_sem=send_b_sem.at[step],
            recv_sem=recv_b_sem.at[step],
            device_id=(row_to, col_to),
            device_id_type=pl.DeviceIdType.MESH,
        )
        copy.start()
        last.append(copy)
    recv_b[col_me, row_me] = send_b[col_me, row_me]

    for copy in gain_sends:
        copy.wait_recv()
    lane = lax.broadcasted_iota(jnp.int32, (rows_n * half, LANES), 1)
    for q in range(cols_n):
        col_gain = column(gains[q], 0, width).reshape(rows_n, own, 1)
        result = jnp.zeros((rows_n * half, LANES), F32)
        for g in range(groups):
            part = col_gain[:, g * half : (g + 1) * half].reshape(rows_n * half, 1)
            result = jnp.where(lax.div(lane, piece) == g, part, result)
        gain_map[q] = result
    for copy in copies[10:]:
        copy.wait()
    for copy in second_sends + last:
        copy.wait_recv()

    group_width = CHANNELS // GROUPS
    per_group = group_width // own
    turned = []
    for q in range(cols_n):
        for r in range(0, rows_n, per_group):
            x = recv_b[q, r : r + per_group].astype(F32).reshape(per_group * half, LANES)
            x = x * recv_s[q, r * half : (r + per_group) * half, :].astype(F32)
            total = jnp.sum(x * x, axis=0, keepdims=True)
            square = total
            for g in range(1, groups):
                square = square + pltpu.roll(total, g * piece, 1)
            scale = lax.rsqrt(square * (1.0 / group_width) + NORM_EPS)
            gain = gain_map[q, r * half : (r + per_group) * half, :]
            turned.append(x * scale * gain)
    mixed = jnp.concatenate(turned, axis=0).T.astype(BF16)
    depth = everyone * half
    step_width = 512
    for start in range(0, out_ref.shape[1], step_width):
        acc = jnp.zeros((piece, step_width), F32)
        for g in range(groups):
            acc = acc + jnp.dot(
                mixed[g * piece : (g + 1) * piece],
                out_w_v[g, :, :, start : start + step_width].reshape(depth, step_width),
                preferred_element_type=F32,
            )
        out_ref[:, start : start + step_width] = acc.astype(BF16)

    for _, copy in sends:
        copy.wait_send()
    for copy in halo_sends + gain_sends + second_sends + last:
        copy.wait_send()


def fast_local(*args):
    (
        tokens, norm_gain, first_gate, second_gate, value_weight, short_weight, short_bias,
        embed_weight, embed_bias, inner_weight, inner_bias, filter_freq, filter_weight,
        filter_skip, output_gain, output_weight,
    ) = args
    rows_n, cols_n = lax.axis_size("row"), lax.axis_size("col")
    block, model = tokens.shape
    own = filter_weight.shape[3]
    piece = block // cols_n
    groups = LANES // piece
    half = own // groups
    tiles = block // LANES
    length = block * rows_n
    width = first_gate.shape[1]
    everyone = rows_n * cols_n
    tables = fast_tables(length, rows_n, tiles, half)
    out_width = output_weight.shape[1]
    out_w = output_weight.reshape(everyone, groups, half, out_width)
    vm = pl.BlockSpec(memory_space=pltpu.VMEM)
    hbm = pl.BlockSpec(memory_space=pl.ANY)
    small = [
        norm_gain.reshape(1, -1),
        short_weight,
        short_bias,
        embed_weight,
        embed_bias.reshape(1, -1),
        inner_weight,
        inner_bias.reshape(1, -1),
        filter_freq.reshape(1, -1),
        jnp.swapaxes(filter_weight, 2, 3),
        filter_skip,
        output_gain.reshape(1, -1),
    ]
    operands = [tokens, first_gate, second_gate, value_weight, out_w, *small, *tables]
    rows_all = tiles * rows_n * half
    DMA = pltpu.SemaphoreType.DMA
    return pl.pallas_call(
        functools.partial(fast_kernel, (rows_n, cols_n, block, own)),
        out_shape=pltpu.VMEM((piece, out_width), BF16),
        in_specs=[hbm] * len(operands),
        out_specs=vm,
        scratch_shapes=[
            pltpu.VMEM(tokens.shape, BF16),
            pltpu.VMEM((3, model, width), BF16),
            pltpu.VMEM((groups, everyone, half, out_width), BF16),
        ]
        + [pltpu.VMEM(array.shape, array.dtype) for array in small + list(tables)]
        + [
            pltpu.VMEM(tokens.shape, BF16),
            pltpu.VMEM((2, rows_n, own, block), BF16),
            pltpu.VMEM((2, rows_n, own, block), BF16),
            pltpu.VMEM((cols_n, rows_n, half, LANES), BF16),
            pltpu.VMEM((cols_n, rows_n, half, LANES), BF16),
            pltpu.VMEM((cols_n, rows_n * half, LANES), BF16),
            pltpu.VMEM((cols_n, rows_n * half, LANES), BF16),
            pltpu.VMEM((width, block), F32),
            pltpu.VMEM((2, 1, width), F32),
            pltpu.VMEM((2, 1, width), F32),
            pltpu.VMEM((cols_n, 1, width), F32),
            pltpu.VMEM((cols_n, rows_n * half, LANES), F32),
            pltpu.VMEM((2, groups, rows_all, 2 * LANES), F32),
            pltpu.VMEM((tables[-1].shape[0] // 3, embed_weight.shape[1]), F32),
            DMA((10 + groups,)),
            DMA((SMALL,)),
            DMA((2, rows_n)),
            DMA((2, rows_n)),
            DMA((everyone,)),
            DMA((everyone,)),
            DMA((cols_n,)),
            DMA((cols_n,)),
            DMA((cols_n,)),
            DMA((cols_n,)),
            DMA((2,)),
            DMA((2,)),
        ],
        compiler_params=pltpu.CompilerParams(
            collective_id=0, has_side_effects=True, vmem_limit_bytes=56 * 1024 * 1024
        ),
    )(*operands)


def kernel_fits(tokens, filter_weight, rows_n, cols_n):
    block = tokens.shape[0]
    own = filter_weight.shape[3]
    piece = block // cols_n
    if block % LANES or LANES % piece:
        return False
    groups = LANES // piece
    return own % (groups * SUBLANES) == 0 and (CHANNELS // GROUPS) % own == 0


def local(*args):
    if kernel_fits(args[0], args[12], lax.axis_size("row"), lax.axis_size("col")):
        return fast_local(*args)
    return general_local(*args)


def solution(mesh):
    in_specs = (
        P("row", None),
        P(),
        P(None, "col"),
        P(None, "col"),
        P(None, "col"),
        P(None, None, "col"),
        P(None, "col"),
        P(),
        P(),
        P(),
        P(),
        P(),
        P(None, None, None, ("col", "row")),
        P(None, ("col", "row")),
        P("col"),
        P(),
    )
    out_specs = P(("row", "col"), None)
    return jax.shard_map(local, mesh=mesh, in_specs=in_specs, out_specs=out_specs, check_vma=False)
```

```python
import functools
import math

import jax
import jax.numpy as jnp
import numpy as np
from jax import lax
from jax.experimental import pallas as pl
from jax.experimental.pallas import tpu as pltpu
from jax.sharding import PartitionSpec as P

CHANNELS = 1024
GROUPS = 8
FREQ_BANDS = 16


HIGHEST = lax.Precision.HIGHEST
NORM_EPS = 1e-06
DECAY_TARGET = 0.01
FAST_SPAN = 0.3
SLOW_SPAN = 1.5


def for_sending(value):
    return jax.tree.map(lambda a: a.astype(jnp.bfloat16) if a.dtype == jnp.float32 else a, value)


def position_features(length):
    position_ramp = jnp.linspace(0.0, 1.0, length, dtype=jnp.float32)[:, None]
    angles = 2.0 * math.pi * jnp.arange(length, dtype=jnp.float32)[:, None] / length
    band_freqs = jnp.linspace(0.0001, FREQ_BANDS - 1, FREQ_BANDS, dtype=jnp.float32)[None, :]
    features = jnp.concatenate(
        [position_ramp, jnp.cos(band_freqs * angles), -jnp.sin(band_freqs * angles)], axis=1
    )
    return (position_ramp, features)


def filter_hidden(length, embed_weight, embed_bias, inner_weight, inner_bias, filter_freq):
    position_ramp, features = position_features(length)
    hidden = jnp.sin(
        filter_freq * (jnp.dot(features, embed_weight, precision=HIGHEST) + embed_bias)
    )
    hidden = jnp.sin(filter_freq * (jnp.dot(hidden, inner_weight, precision=HIGHEST) + inner_bias))
    return (position_ramp, hidden)


def decay_rates():
    fastest = math.log(DECAY_TARGET) / FAST_SPAN
    slowest = math.log(DECAY_TARGET) / SLOW_SPAN
    return jnp.abs(jnp.linspace(slowest, fastest, CHANNELS, dtype=jnp.float32))


def short_filter(padded, weights, bias_row, length):
    result = bias_row.astype(jnp.float32)
    for tap_index in range(weights.shape[0]):
        result = result + padded[tap_index : tap_index + length].astype(jnp.float32) * weights[
            tap_index
        ].astype(jnp.float32)
    return result


def phase_table(rows, cols, period):
    phase_index = (
        lax.broadcasted_iota(jnp.int32, (rows, cols), 0)
        * lax.broadcasted_iota(jnp.int32, (rows, cols), 1)
        % period
    )
    phase_angle = phase_index.astype(jnp.float32) * (2.0 * math.pi / period)
    return (jnp.cos(phase_angle), jnp.sin(phase_angle))


def split_length(total_size):
    chosen = 2
    for candidate in range(2, math.isqrt(total_size) + 1, 2):
        if total_size % candidate == 0:
            chosen = candidate
    return chosen


def make_tables(total_size):
    major_size = split_length(total_size)
    minor_size = total_size // major_size
    inner_table = phase_table(major_size, major_size, major_size)
    twiddle = phase_table(major_size, minor_size, total_size)
    outer_table = phase_table(minor_size, minor_size, minor_size)
    return (major_size, minor_size, inner_table, twiddle, outer_table)


def finish_forward(part_real, part_imag, twiddle, outer_table):
    turn_cos = twiddle[0][:, :, None]
    turn_sin = twiddle[1][:, :, None]
    turned_real = part_real * turn_cos + part_imag * turn_sin
    turned_imag = part_imag * turn_cos - part_real * turn_sin
    outer_cos, outer_sin = outer_table
    spec_real = jnp.einsum("anc,nk->akc", turned_real, outer_cos, precision=HIGHEST) + jnp.einsum(
        "anc,nk->akc", turned_imag, outer_sin, precision=HIGHEST
    )
    spec_imag = jnp.einsum("anc,nk->akc", turned_imag, outer_cos, precision=HIGHEST) - jnp.einsum(
        "anc,nk->akc", turned_real, outer_sin, precision=HIGHEST
    )
    return (spec_real, spec_imag)


def forward_signal(signal, tables):
    major_size, minor_size, inner_table, twiddle, outer_table = tables
    channels = signal.shape[1]
    flattened = signal.reshape(major_size // 2, minor_size * channels)
    inner_cos = inner_table[0][:, : major_size // 2]
    inner_sin = inner_table[1][:, : major_size // 2]
    part_real = jnp.dot(inner_cos, flattened, precision=HIGHEST).reshape(
        major_size, minor_size, channels
    )
    part_imag = -jnp.dot(inner_sin, flattened, precision=HIGHEST).reshape(
        major_size, minor_size, channels
    )
    return finish_forward(part_real, part_imag, twiddle, outer_table)


def forward_taps(circular_taps, tables):
    major_size, minor_size, inner_table, twiddle, outer_table = tables
    channels = circular_taps.shape[1]
    flattened = circular_taps.reshape(major_size, minor_size * channels)
    part_real = jnp.dot(inner_table[0], flattened, precision=HIGHEST).reshape(
        major_size, minor_size, channels
    )
    part_imag = -jnp.dot(inner_table[1], flattened, precision=HIGHEST).reshape(
        major_size, minor_size, channels
    )
    return finish_forward(part_real, part_imag, twiddle, outer_table)


def inverse(spec_real, spec_imag, tables):
    major_size, minor_size, inner_table, twiddle, outer_table = tables
    channels = spec_real.shape[2]
    outer_cos, outer_sin = outer_table
    back_real = jnp.einsum("akc,kn->anc", spec_real, outer_cos, precision=HIGHEST) - jnp.einsum(
        "akc,kn->anc", spec_imag, outer_sin, precision=HIGHEST
    )
    back_imag = jnp.einsum("akc,kn->anc", spec_imag, outer_cos, precision=HIGHEST) + jnp.einsum(
        "akc,kn->anc", spec_real, outer_sin, precision=HIGHEST
    )
    turn_cos = twiddle[0][:, :, None]
    turn_sin = twiddle[1][:, :, None]
    turned_real = (back_real * turn_cos - back_imag * turn_sin).reshape(
        major_size, minor_size * channels
    )
    turned_imag = (back_imag * turn_cos + back_real * turn_sin).reshape(
        major_size, minor_size * channels
    )
    half_rows = major_size // 2
    values = jnp.dot(inner_table[0][:half_rows], turned_real, precision=HIGHEST) - jnp.dot(
        inner_table[1][:half_rows], turned_imag, precision=HIGHEST
    )
    return values.reshape(half_rows * minor_size, channels) / (major_size * minor_size)


def two_sided(signal, forward, backward, skip_gain, tables):
    circular_taps = jnp.concatenate([forward, jnp.zeros_like(forward[:1]), backward[:0:-1]], axis=0)
    signal_real, signal_imag = forward_signal(signal, tables)
    taps_real, taps_imag = forward_taps(circular_taps, tables)
    prod_real = signal_real * taps_real - signal_imag * taps_imag
    prod_imag = signal_real * taps_imag + signal_imag * taps_real
    return inverse(prod_real, prod_imag, tables) + signal * skip_gain


def channel_taps(hidden, position_ramp, filter_weight, deltas):
    window = jnp.exp(-position_ramp * deltas[None, :])
    pairs = []
    for order_index in range(filter_weight.shape[0]):
        forward = jnp.dot(hidden, filter_weight[order_index, 0], precision=HIGHEST) * window
        backward = jnp.dot(hidden, filter_weight[order_index, 1], precision=HIGHEST) * window
        pairs.append((forward, backward))
    return pairs


def general_local(
    tokens,
    norm_gain,
    first_gate,
    second_gate,
    value_weight,
    short_weight,
    short_bias,
    embed_weight,
    embed_bias,
    inner_weight,
    inner_bias,
    filter_freq,
    filter_weight,
    filter_skip,
    output_gain,
    output_weight,
):
    row_count = lax.axis_size("row")
    row_index = lax.axis_index("row")
    col_index = lax.axis_index("col")
    local_tokens = tokens.shape[0]
    length = local_tokens * row_count
    col_width = first_gate.shape[1]
    own_width = col_width // row_count
    widened = tokens.astype(jnp.float32)
    normed = (
        widened
        * lax.rsqrt(jnp.mean(widened * widened, axis=1, keepdims=True) + NORM_EPS)
        * norm_gain
    ).astype(jnp.bfloat16)
    gate_first = jnp.dot(normed, first_gate, preferred_element_type=jnp.float32).astype(
        jnp.bfloat16
    )
    gate_second = jnp.dot(normed, second_gate, preferred_element_type=jnp.float32).astype(
        jnp.bfloat16
    )
    gate_value = jnp.dot(normed, value_weight, preferred_element_type=jnp.float32).astype(
        jnp.bfloat16
    )
    position_ramp, hidden = filter_hidden(
        length, embed_weight, embed_bias, inner_weight, inner_bias, filter_freq
    )
    channel_start = (col_index * row_count + row_index) * own_width
    deltas = lax.dynamic_slice_in_dim(decay_rates(), channel_start, own_width)
    tap_pairs = channel_taps(hidden, position_ramp, filter_weight, deltas)
    tables = make_tables(2 * length)
    half_width = short_weight.shape[1] // 2
    moved = (
        lax.all_to_all(gate_first, "row", split_axis=1, concat_axis=0, tiled=True),
        lax.all_to_all(gate_second, "row", split_axis=1, concat_axis=0, tiled=True),
        lax.all_to_all(gate_value, "row", split_axis=1, concat_axis=0, tiled=True),
    )
    weights_own = lax.dynamic_slice_in_dim(short_weight, row_index * own_width, own_width, 2)
    bias_own = lax.dynamic_slice_in_dim(short_bias, row_index * own_width, own_width, 1)
    smoothed = [
        short_filter(
            jnp.pad(moved[branch], ((half_width, half_width), (0, 0))),
            weights_own[branch],
            bias_own[branch],
            length,
        )
        for branch in range(3)
    ]
    signal = smoothed[2]
    for order_index in range(2):
        signal = smoothed[order_index] * two_sided(
            signal,
            tap_pairs[order_index][0],
            tap_pairs[order_index][1],
            filter_skip[order_index],
            tables,
        )
    result = jax.tree.map(
        lambda part, own: part.astype(own.dtype),
        lax.all_to_all(for_sending(signal), "row", split_axis=0, concat_axis=1, tiled=True),
        signal,
    )
    group_width = CHANNELS // GROUPS
    grouped = result.reshape(local_tokens, col_width // group_width, group_width)
    scaled = grouped * lax.rsqrt(jnp.mean(grouped * grouped, axis=2, keepdims=True) + NORM_EPS)
    mix_local = (scaled.reshape(local_tokens, col_width) * output_gain).astype(jnp.bfloat16)
    gathered = lax.all_to_all(mix_local, "col", split_axis=0, concat_axis=1, tiled=True)
    return jnp.dot(gathered, output_weight, preferred_element_type=jnp.float32).astype(jnp.bfloat16)


LANES = 128
SUBLANES = 16
BF16 = jnp.bfloat16
F32 = jnp.float32


def fast_tables(length, rows, tile_rows, own):
    total = 2 * length
    majors = length // LANES
    n1 = (np.arange(rows)[None, :] * tile_rows + np.arange(tile_rows)[:, None]).reshape(-1)
    k1 = np.arange(majors) + 0.5
    angle = 2.0 * np.pi * np.outer(k1, n1) / (2 * majors)
    eye = np.eye(own)
    inner = np.concatenate([np.kron(np.cos(angle), eye), np.kron(-np.sin(angle), eye)], 0)
    inner_back = inner.T * (2.0 / total)
    n2 = np.arange(LANES)
    turn = np.repeat(2.0 * np.pi * np.outer(k1, n2) / total, own, axis=0)
    twiddle = np.stack([np.cos(turn), np.sin(turn)])
    phase = 2.0 * np.pi * (np.outer(n2, n2) % LANES) / LANES
    c, s = np.cos(phase), np.sin(phase)
    outer = np.block([[c, -s], [s, c]])
    ramp = np.linspace(0.0, 1.0, length)
    angles = 2.0 * np.pi * np.arange(length) / length
    bands = np.linspace(0.0001, FREQ_BANDS - 1, FREQ_BANDS)[:, None]
    feats = np.concatenate([ramp[None], np.cos(bands * angles), -np.sin(bands * angles)], 0)
    feats = np.pad(feats, ((0, -feats.shape[0] % SUBLANES), (0, 0))).astype(np.float32)
    high = feats.astype(BF16)
    low = (feats - high.astype(np.float32)).astype(BF16)
    return (
        jnp.asarray(inner, BF16),
        jnp.asarray(inner_back, BF16),
        jnp.asarray(twiddle, F32),
        jnp.asarray(outer, BF16),
        jnp.asarray(outer.T, BF16),
        jnp.asarray(np.concatenate([high, low, high], 0)),
    )


def bounded_sin(x):
    turns = jnp.round(x * (1.0 / math.pi))
    r = x - turns * 3.140625
    r = r - turns * 9.67502593994140625e-4
    r = r - turns * 1.509957990978376432e-7
    half = turns * 0.5
    sign = 1.0 - 4.0 * (half - jnp.floor(half))
    q = r * r
    p = -2.5052108385e-8 + q * 1.6059043837e-10
    p = 2.7557319224e-6 + q * p
    p = -1.9841269841e-4 + q * p
    p = 8.3333333333e-3 + q * p
    p = -1.6666666667e-1 + q * p
    return sign * (r + r * q * p)


def mm(a, b):
    return jnp.dot(a.astype(BF16), b.astype(BF16), preferred_element_type=F32)


def halves(x):
    high = x.astype(BF16).astype(F32)
    return high, x - high


def tdot(a, stacked):
    high, low = halves(a)
    return lax.dot_general(
        jnp.concatenate([high, high, low], 0).astype(BF16),
        stacked,
        (((0,), (0,)), ((), ())),
        preferred_element_type=F32,
    )


def stack(b):
    high, low = halves(b)
    return jnp.concatenate([high, low, high], 0).astype(BF16)


def column(row, start, count):
    shape = (count, row.shape[1])
    hit = lax.broadcasted_iota(jnp.int32, shape, 1) == start + lax.broadcasted_iota(
        jnp.int32, shape, 0
    )
    return jnp.sum(jnp.where(hit, row.astype(F32), 0.0), axis=1, keepdims=True)


SMALL = 11


def fast_kernel(dims, *refs):
    tokens_h, first_h, second_h, value_h, out_w_h = refs[:5]
    small_h = refs[5 : 5 + SMALL]
    inner_h, inner_back_h, twiddle_h, outer_h, outer_back_h, feats_h, out_ref = refs[
        5 + SMALL : 12 + SMALL
    ]
    tokens_v, gates_v, out_w_v = refs[12 + SMALL : 15 + SMALL]
    small_v = refs[15 + SMALL : 15 + 2 * SMALL]
    (
        norm_gain, short_weight, short_bias, embed_weight, embed_bias, inner_weight,
        inner_bias, filter_freq, filter_weight, filter_skip, output_gain,
    ) = small_v
    (
        inner_v, inner_back_v, twiddle_v, outer_v, outer_back_v, feats_v, normed_v,
        send_a, recv_a, send_b, recv_b, send_s, recv_s, second_v, send_h, recv_h, gains,
        gain_map, spectra, embed_pad, load_sem, small_sem, send_a_sem, recv_a_sem, send_b_sem,
        recv_b_sem, send_g_sem, recv_g_sem, send_s_sem, recv_s_sem, send_h_sem, recv_h_sem,
    ) = refs[15 + 2 * SMALL :]
    rows_n, cols_n, block, own = dims
    length = rows_n * block
    tiles = block // LANES
    piece = block // cols_n
    groups = LANES // piece
    half = own // groups
    row_me = lax.axis_index("row")
    col_me = lax.axis_index("col")
    me = row_me * cols_n + col_me
    everyone = rows_n * cols_n

    loads = [
        (tokens_h, tokens_v),
        (value_h, gates_v.at[2]),
        (first_h, gates_v.at[0]),
        (second_h, gates_v.at[1]),
        (feats_h, feats_v),
        (inner_h, inner_v),
        (twiddle_h, twiddle_v),
        (outer_h, outer_v),
        (outer_back_h, outer_back_v),
        (inner_back_h, inner_back_v),
    ] + [(out_w_h.at[:, g], out_w_v.at[g]) for g in range(groups)]
    copies = [
        pltpu.make_async_copy(src, dst, load_sem.at[i]) for i, (src, dst) in enumerate(loads)
    ]
    smalls = [
        pltpu.make_async_copy(src, dst, small_sem.at[i])
        for i, (src, dst) in enumerate(zip(small_h, small_v))
    ]
    copies[0].start()
    smalls[0].start()
    copies[1].start()

    def place(flat):
        return (lax.div(flat, cols_n), lax.rem(flat, cols_n))

    barrier = pltpu.get_barrier_semaphore()
    for step in range(1, everyone):
        pl.semaphore_signal(
            barrier,
            inc=1,
            device_id=place(lax.rem(me + step, everyone)),
            device_id_type=pl.DeviceIdType.MESH,
        )

    for copy in copies[2:10] + smalls[1:]:
        copy.start()
    copies[0].wait()
    smalls[0].wait()
    gain_row = norm_gain[...]
    chunk = 32
    for start in range(0, block, chunk):
        x = tokens_v[start : start + chunk, :].astype(F32)
        scale = lax.rsqrt(jnp.mean(x * x, axis=1, keepdims=True) + NORM_EPS)
        normed_v[start : start + chunk, :] = (x * scale * gain_row).astype(BF16)

    MESH = pl.DeviceIdType.MESH
    sends = []

    def project(order, branch):
        copies[1 + order].wait()
        gate = jnp.dot(normed_v[...], gates_v[branch], preferred_element_type=F32)
        send_a[order] = gate.T.astype(BF16).reshape(rows_n, own, block)
        if order == 0:
            pl.semaphore_wait(barrier, everyone - 1)
        for step in range(1, rows_n):
            peer = lax.rem(row_me + step, rows_n)
            copy = pltpu.make_async_remote_copy(
                src_ref=send_a.at[order, peer],
                dst_ref=recv_a.at[order, row_me],
                send_sem=send_a_sem.at[order, step],
                recv_sem=recv_a_sem.at[order, step],
                device_id=(peer, col_me),
                device_id_type=MESH,
            )
            copy.start()
            sends.append((order, copy))
        recv_a[order, row_me] = send_a[order, row_me]

    project(0, 2)
    project(1, 0)
    copies[3].wait()
    gate = jnp.dot(normed_v[...], gates_v[1], preferred_element_type=F32)
    gate = gate.astype(BF16).astype(F32)
    second_v[...] = gate.T
    send_h[0] = gate[:1]
    send_h[1] = gate[block - 1 :]
    halo_sends = []
    for edge, shift in ((0, rows_n - 1), (1, 1)):
        copy = pltpu.make_async_remote_copy(
            src_ref=send_h.at[edge],
            dst_ref=recv_h.at[edge],
            send_sem=send_h_sem.at[edge],
            recv_sem=recv_h_sem.at[edge],
            device_id=(lax.rem(row_me + shift, rows_n), col_me),
            device_id_type=MESH,
        )
        copy.start()
        halo_sends.append(copy)
    for copy in copies[10:]:
        copy.start()
    for copy in smalls[1:]:
        copy.wait()

    gain_sends = []
    gains[col_me] = output_gain[...]
    for step in range(1, cols_n):
        copy = pltpu.make_async_remote_copy(
            src_ref=output_gain,
            dst_ref=gains.at[col_me],
            send_sem=send_g_sem.at[step],
            recv_sem=recv_g_sem.at[step],
            device_id=(row_me, lax.rem(col_me + step, cols_n)),
            device_id_type=pl.DeviceIdType.MESH,
        )
        copy.start()
        gain_sends.append(copy)

    def to_layout(x):
        return jnp.concatenate(
            [
                jnp.concatenate(
                    [
                        x[:, g * half : (g + 1) * half, j * LANES : (j + 1) * LANES].reshape(
                            rows_n * half, LANES
                        )
                        for g in range(groups)
                    ],
                    axis=1,
                )
                for j in range(tiles)
            ],
            axis=0,
        )

    def taps_layout(x):
        return jnp.concatenate(
            [
                jnp.concatenate(
                    [
                        x[
                            g * half : (g + 1) * half,
                            (r * tiles + j) * LANES : (r * tiles + j + 1) * LANES,
                        ]
                        for g in range(groups)
                    ],
                    axis=1,
                )
                for j in range(tiles)
                for r in range(rows_n)
            ],
            axis=0,
        )

    freq = column(filter_freq[...], 0, filter_freq.shape[1])
    copies[4].wait()
    embed_pad[...] = jnp.zeros_like(embed_pad)
    embed_pad[: embed_weight.shape[0], :] = embed_weight[...]
    hidden = bounded_sin(
        freq
        * (
            tdot(embed_pad[...], feats_v[...])
            + column(embed_bias[...], 0, embed_bias.shape[1])
        )
    )
    hidden = bounded_sin(
        freq * (tdot(inner_weight[...], stack(hidden)) + column(inner_bias[...], 0, inner_bias.shape[1]))
    )
    channels = rows_n * cols_n * own
    slowest = math.log(DECAY_TARGET) / SLOW_SPAN
    fastest = math.log(DECAY_TARGET) / FAST_SPAN
    channel = (
        (col_me * rows_n + row_me) * own + lax.broadcasted_iota(jnp.int32, (own, 1), 0)
    ).astype(F32)
    decay = jnp.abs(slowest + channel * ((fastest - slowest) / (channels - 1)))
    lag = lax.broadcasted_iota(jnp.int32, (own, length), 1)
    window = jnp.exp(-(lag.astype(F32) * (1.0 / (length - 1))) * decay)
    for copy in copies[5:8]:
        copy.wait()

    def twist(real, imag, sign):
        cos = jnp.concatenate([twiddle_v[0]] * groups, axis=1)
        sin = jnp.concatenate([twiddle_v[1]] * groups, axis=1) * sign
        return real * cos + imag * sin, imag * cos - real * sin

    def lanes_of(x, g):
        return x[:, g * LANES : (g + 1) * LANES]

    def forward_inner(x):
        part = mm(inner_v[...], x)
        count = part.shape[0] // 2
        return twist(part[:count], part[count:], 1.0)

    high, low = halves(filter_weight[...].reshape(4 * own, filter_weight.shape[3]))
    taps = jnp.dot(
        jnp.concatenate([high, high, low], 1).astype(BF16),
        stack(hidden),
        preferred_element_type=F32,
    )
    for order in range(2):
        fwd = taps[2 * order * own : (2 * order + 1) * own] * window
        bwd = taps[(2 * order + 1) * own : (2 * order + 2) * own] * window
        bwd = jnp.where(lag == 0, 0.0, bwd)
        plus = forward_inner(taps_layout(fwd + bwd))
        minus = forward_inner(taps_layout(fwd - bwd))
        for g in range(groups):
            p = jnp.concatenate([lanes_of(plus[0], g), lanes_of(plus[1], g)], axis=1)
            m = jnp.concatenate([lanes_of(minus[0], g), lanes_of(minus[1], g)], axis=1)
            spectra[order, g, :, :LANES] = mm(p, outer_v[:, :LANES])
            spectra[order, g, :, LANES:] = mm(m, outer_v[:, LANES:])

    width = rows_n * own
    count = rows_n * half
    second_sends = []

    def send_second():
        for copy in halo_sends:
            copy.wait_recv()
        x = second_v[...]
        spot = lax.broadcasted_iota(jnp.int32, (width, block), 1)
        first_col = jnp.where(row_me == 0, 0.0, column(recv_h[1], 0, width))
        last_col = jnp.where(row_me == rows_n - 1, 0.0, column(recv_h[0], 0, width))
        before = jnp.where(spot == 0, first_col, pltpu.roll(x, 1, 1))
        after = jnp.where(spot == block - 1, last_col, pltpu.roll(x, block - 1, 1))
        w = [column(short_weight[1, j : j + 1, :], 0, width) for j in range(3)]
        x = column(short_bias[1:2, :], 0, width) + before * w[0] + x * w[1] + after * w[2]
        x = x.reshape(rows_n, groups, half, block)
        for q in range(cols_n):
            part = jnp.concatenate(
                [x[:, g, :, q * piece : (q + 1) * piece].reshape(count, piece) for g in range(groups)],
                axis=1,
            )
            send_s[q] = part.astype(BF16)
        recv_s[col_me] = send_s[col_me]
        for step in range(1, cols_n):
            peer = lax.rem(col_me + step, cols_n)
            copy = pltpu.make_async_remote_copy(
                src_ref=send_s.at[peer],
                dst_ref=recv_s.at[col_me],
                send_sem=send_s_sem.at[step],
                recv_sem=recv_s_sem.at[step],
                device_id=(row_me, peer),
                device_id_type=MESH,
            )
            copy.start()
            second_sends.append(copy)

    for copy in copies[8:10]:
        copy.wait()
    pos = lax.broadcasted_iota(jnp.int32, (rows_n, own, block), 2)

    def smooth(slot, branch):
        for b, copy in sends:
            if b == slot:
                copy.wait_recv()
        x = recv_a[slot].astype(F32)
        flat = x.reshape(rows_n * own, block)
        before = pltpu.roll(flat, 1, 1).reshape(rows_n, own, block)
        after = pltpu.roll(flat, block - 1, 1).reshape(rows_n, own, block)
        gap = jnp.zeros((1, own, block), F32)
        before = jnp.where(pos == 0, jnp.concatenate([gap, before[:-1]], 0), before)
        after = jnp.where(pos == block - 1, jnp.concatenate([after[1:], gap], 0), after)
        start = row_me * own
        w = [
            column(short_weight[branch, j : j + 1, :], start, own).reshape(1, own, 1)
            for j in range(3)
        ]
        bias = column(short_bias[branch : branch + 1, :], start, own).reshape(1, own, 1)
        return to_layout(bias + before * w[0] + x * w[1] + after * w[2])

    signal = smooth(0, 2)
    for order in range(2):
        real, imag = forward_inner(signal)
        back_real, back_imag = [], []
        for g in range(groups):
            t = jnp.concatenate([lanes_of(real, g), lanes_of(imag, g)], axis=1)
            spec = mm(t, outer_v[...])
            sr, si = spec[:, :LANES], spec[:, LANES:]
            hr, hi = spectra[order, g, :, :LANES], spectra[order, g, :, LANES:]
            prod = jnp.concatenate([sr * hr - si * hi, sr * hi + si * hr], axis=1)
            back = mm(prod, outer_back_v[...])
            back_real.append(back[:, :LANES])
            back_imag.append(back[:, LANES:])
        ur, ui = twist(jnp.concatenate(back_real, 1), jnp.concatenate(back_imag, 1), -1.0)
        conv = mm(inner_back_v[...], jnp.concatenate([ur, ui], axis=0))
        skip = column(filter_skip[order : order + 1, :], 0, own)
        skip = to_layout(jnp.broadcast_to(skip[None], (rows_n, own, block)))
        signal = conv + signal * skip
        if order == 0:
            signal = signal * smooth(1, 0)

    for j in range(tiles):
        for h in range(LANES // piece):
            part = jnp.concatenate(
                [
                    signal[
                        j * count : (j + 1) * count,
                        g * LANES + h * piece : g * LANES + (h + 1) * piece,
                    ]
                    for g in range(groups)
                ],
                axis=1,
            )
            send_b[j * (LANES // piece) + h] = part.astype(BF16).reshape(rows_n, half, LANES)
    last = []
    for step in range(1, everyone):
        row_to, col_to = place(lax.rem(me + step, everyone))
        copy = pltpu.make_async_remote_copy(
            src_ref=send_b.at[col_to, row_to],
            dst_ref=recv_b.at[col_me, row_me],
            send_sem=send_b_sem.at[step],
            recv_sem=recv_b_sem.at[step],
            device_id=(row_to, col_to),
            device_id_type=pl.DeviceIdType.MESH,
        )
        copy.start()
        last.append(copy)
    recv_b[col_me, row_me] = send_b[col_me, row_me]
    send_second()

    for copy in gain_sends:
        copy.wait_recv()
    lane = lax.broadcasted_iota(jnp.int32, (rows_n * half, LANES), 1)
    for q in range(cols_n):
        col_gain = column(gains[q], 0, width).reshape(rows_n, own, 1)
        result = jnp.zeros((rows_n * half, LANES), F32)
        for g in range(groups):
            part = col_gain[:, g * half : (g + 1) * half].reshape(rows_n * half, 1)
            result = jnp.where(lax.div(lane, piece) == g, part, result)
        gain_map[q] = result
    for copy in copies[10:]:
        copy.wait()
    for copy in second_sends + last:
        copy.wait_recv()

    group_width = CHANNELS // GROUPS
    per_group = group_width // own
    turned = []
    for q in range(cols_n):
        for r in range(0, rows_n, per_group):
            x = recv_b[q, r : r + per_group].astype(F32).reshape(per_group * half, LANES)
            x = x * recv_s[q, r * half : (r + per_group) * half, :].astype(F32)
            total = jnp.sum(x * x, axis=0, keepdims=True)
            square = total
            for g in range(1, groups):
                square = square + pltpu.roll(total, g * piece, 1)
            scale = lax.rsqrt(square * (1.0 / group_width) + NORM_EPS)
            gain = gain_map[q, r * half : (r + per_group) * half, :]
            turned.append(x * scale * gain)
    mixed = jnp.concatenate(turned, axis=0).T.astype(BF16)
    depth = everyone * half
    step_width = 512
    for start in range(0, out_ref.shape[1], step_width):
        acc = jnp.zeros((piece, step_width), F32)
        for g in range(groups):
            acc = acc + jnp.dot(
                mixed[g * piece : (g + 1) * piece],
                out_w_v[g, :, :, start : start + step_width].reshape(depth, step_width),
                preferred_element_type=F32,
            )
        out_ref[:, start : start + step_width] = acc.astype(BF16)

    for _, copy in sends:
        copy.wait_send()
    for copy in halo_sends + gain_sends + second_sends + last:
        copy.wait_send()


def fast_local(*args):
    (
        tokens, norm_gain, first_gate, second_gate, value_weight, short_weight, short_bias,
        embed_weight, embed_bias, inner_weight, inner_bias, filter_freq, filter_weight,
        filter_skip, output_gain, output_weight,
    ) = args
    rows_n, cols_n = lax.axis_size("row"), lax.axis_size("col")
    block, model = tokens.shape
    own = filter_weight.shape[3]
    piece = block // cols_n
    groups = LANES // piece
    half = own // groups
    tiles = block // LANES
    length = block * rows_n
    width = first_gate.shape[1]
    everyone = rows_n * cols_n
    tables = fast_tables(length, rows_n, tiles, half)
    out_width = output_weight.shape[1]
    out_w = output_weight.reshape(everyone, groups, half, out_width)
    vm = pl.BlockSpec(memory_space=pltpu.VMEM)
    hbm = pl.BlockSpec(memory_space=pl.ANY)
    small = [
        norm_gain.reshape(1, -1),
        short_weight,
        short_bias,
        embed_weight,
        embed_bias.reshape(1, -1),
        inner_weight,
        inner_bias.reshape(1, -1),
        filter_freq.reshape(1, -1),
        jnp.swapaxes(filter_weight, 2, 3),
        filter_skip,
        output_gain.reshape(1, -1),
    ]
    operands = [tokens, first_gate, second_gate, value_weight, out_w, *small, *tables]
    rows_all = tiles * rows_n * half
    DMA = pltpu.SemaphoreType.DMA
    return pl.pallas_call(
        functools.partial(fast_kernel, (rows_n, cols_n, block, own)),
        out_shape=pltpu.VMEM((piece, out_width), BF16),
        in_specs=[hbm] * len(operands),
        out_specs=vm,
        scratch_shapes=[
            pltpu.VMEM(tokens.shape, BF16),
            pltpu.VMEM((3, model, width), BF16),
            pltpu.VMEM((groups, everyone, half, out_width), BF16),
        ]
        + [pltpu.VMEM(array.shape, array.dtype) for array in small + list(tables)]
        + [
            pltpu.VMEM(tokens.shape, BF16),
            pltpu.VMEM((2, rows_n, own, block), BF16),
            pltpu.VMEM((2, rows_n, own, block), BF16),
            pltpu.VMEM((cols_n, rows_n, half, LANES), BF16),
            pltpu.VMEM((cols_n, rows_n, half, LANES), BF16),
            pltpu.VMEM((cols_n, rows_n * half, LANES), BF16),
            pltpu.VMEM((cols_n, rows_n * half, LANES), BF16),
            pltpu.VMEM((width, block), F32),
            pltpu.VMEM((2, 1, width), F32),
            pltpu.VMEM((2, 1, width), F32),
            pltpu.VMEM((cols_n, 1, width), F32),
            pltpu.VMEM((cols_n, rows_n * half, LANES), F32),
            pltpu.VMEM((2, groups, rows_all, 2 * LANES), F32),
            pltpu.VMEM((tables[-1].shape[0] // 3, embed_weight.shape[1]), F32),
            DMA((10 + groups,)),
            DMA((SMALL,)),
            DMA((2, rows_n)),
            DMA((2, rows_n)),
            DMA((everyone,)),
            DMA((everyone,)),
            DMA((cols_n,)),
            DMA((cols_n,)),
            DMA((cols_n,)),
            DMA((cols_n,)),
            DMA((2,)),
            DMA((2,)),
        ],
        compiler_params=pltpu.CompilerParams(
            collective_id=0, has_side_effects=True, vmem_limit_bytes=56 * 1024 * 1024
        ),
    )(*operands)


def kernel_fits(tokens, filter_weight, rows_n, cols_n):
    block = tokens.shape[0]
    own = filter_weight.shape[3]
    piece = block // cols_n
    if block % LANES or LANES % piece:
        return False
    groups = LANES // piece
    return own % (groups * SUBLANES) == 0 and (CHANNELS // GROUPS) % own == 0


def local(*args):
    if kernel_fits(args[0], args[12], lax.axis_size("row"), lax.axis_size("col")):
        return fast_local(*args)
    return general_local(*args)


def solution(mesh):
    in_specs = (
        P("row", None),
        P(),
        P(None, "col"),
        P(None, "col"),
        P(None, "col"),
        P(None, None, "col"),
        P(None, "col"),
        P(),
        P(),
        P(),
        P(),
        P(),
        P(None, None, None, ("col", "row")),
        P(None, ("col", "row")),
        P("col"),
        P(),
    )
    out_specs = P(("row", "col"), None)
    return jax.shard_map(local, mesh=mesh, in_specs=in_specs, out_specs=out_specs, check_vma=False)
```
